512 devices in a mesh: gr: 2 (over z_hi), sp: 32 (over z_lo, y), tp: 8 (over x, core).
Axes of the slice: x: 4, y: 8, z: 8 (z_hi: 2, z_lo: 4; z = z_hi * 4 + z_lo), core: 2. Of those that a mesh axis runs over, the one named last changes fastest.
Arguments:
- prompt_elements: bfloat16 [4, 8192, 2048], P('gr', 'sp'), may hold values from -6 to 6
- address_weights: bfloat16 [2048, 1024], P(None, 'tp'), may hold values from -0.125 to 0.125
- content_weights: bfloat16 [2048, 1024], P(None, 'tp'), may hold values from -0.125 to 0.125
- lookup_weights: bfloat16 [2048, 1024], P(None, 'tp'), may hold values from -0.125 to 0.125
- forgetting_weights: bfloat16 [2048, 8], replicated, may hold values from -0.125 to 0.125
- update_intensity_weights: bfloat16 [2048, 8], replicated, may hold values from -0.125 to 0.125
- forgetting_speeds: float32 [8], P('tp'), may hold values from 1.2207031e-05 to 0.05, as said below
- update_intensity_ceiling: float32 [8], P('tp'), may hold values from 0.0078125 to 0.03125, as said below
- forgetting_multiplier: float32 [4, 8192, 8], P('gr', 'sp', 'tp'), may hold values from 0.35 to 2.8, as said below
- spike_offsets: float32 [4, 8192, 8], P('gr', 'sp', 'tp'), may hold values from -0.7 to 0, as said below
- upcoming_element_vector: bfloat16 [4, 2048], P('gr'), may hold values from -6 to 6
- retrieval_rms_multiplier: float32 [128], replicated, may hold values from 0.1 to 1.9
Outputs:
- cache: bfloat16 [4, 8, 128, 128], P('gr', 'tp', 'sp')
- read: bfloat16 [4, 1024], P('gr', 'tp')
The draws below stay inside these ranges and needn't reach their ends.
Inputs may be any that keep to these rules, and one draw needn't show every extreme that they name: `forgetting_speeds`: per-head rates of decay. `update_intensity_ceiling`: per-head strength scales. `forgetting_multiplier`: positive factors. `spike_offsets`: non-positive log factors.
All inputs are finite; a program needn't handle non-finite values.
Results may differ from the reference program's by a relative error of at most 0.0037.
Values sent between devices are 32-bit elements; how exact they have to be, the bound alone decides.
A program may use at most 64 MiB of HBM per device.

```python
import math
import jax
import jax.numpy as jnp
from jax import lax

D = 2048
H = 8
DK = 128
BLK = 64
SPAN = 256
NSEQ = 4
LEN = 8192


def draw_forgetting_speeds(key, part):
    order_key, level_key = jax.random.split(jax.random.fold_in(key, 17))
    ranks = jax.random.permutation(order_key, H)
    slow = ranks < H // 2
    level = jax.random.uniform(level_key, (H,), jnp.float32)
    slow_rate = (0.1 + 0.4 * level) / LEN
    fast_rate = 0.02 + 0.03 * level
    return jnp.where(slow, slow_rate, fast_rate).astype(jnp.float32)


def draw_update_intensity_ceiling(key, part):
    level = jax.random.uniform(jax.random.fold_in(key, 19), (H,), jnp.float32, math.log(0.5), math.log(2.0))
    return (jnp.exp(level) * DK / LEN).astype(jnp.float32)


def draw_forgetting_multiplier(key, part):
    bottom, top = (0.5, 2.0)
    level = jax.random.uniform(jax.random.fold_in(key, 23), (NSEQ, LEN // SPAN, H), jnp.float32, math.log(bottom), math.log(top))
    return jnp.repeat(jnp.exp(level), SPAN, axis=1).astype(jnp.float32)


def draw_spike_offsets(key, part):
    hit_key, depth_key = jax.random.split(jax.random.fold_in(key, 29))
    hits = jax.random.uniform(hit_key, (NSEQ, LEN, H), jnp.float32) < 4.0 / LEN
    depth = jax.random.uniform(depth_key, (NSEQ, LEN, H), jnp.float32, math.log(0.5), math.log(0.8))
    return jnp.where(hits, depth, 0.0).astype(jnp.float32)


def level_of(stream_key, extent, cuts, smallest, high):
    gain = 1.0
    for position, blocks in cuts:
        heights = jax.random.uniform(jax.random.fold_in(jax.random.fold_in(stream_key, 6), position), (blocks,), jnp.float32, smallest / len(cuts), high / len(cuts))
        gain = gain * jnp.repeat(jnp.exp(heights), extent[position] // blocks).reshape((-1,) + (1,) * (len(extent) - 1 - position))
    return gain


def bell_draw(own_key, extent, scale, bound, cuts=(), held_as=jnp.bfloat16):
    values = jax.random.normal(own_key, extent, jnp.float32) * scale
    if len(cuts) > 0:
        values = level_of(own_key, extent, cuts, -0.22, 0.18) * values
    return jnp.clip(values, min=-bound, max=bound).astype(held_as)


def setup_inputs(seed: int = 0) -> dict:
    key_list = jax.random.split(jax.random.key(seed), 13)
    prompt_elements = bell_draw(key_list[0], (NSEQ, LEN, D), 1.0, 6.0, ((0, 2), (1, 32)))
    address_weights = bell_draw(key_list[1], (D, H * DK), D ** -0.5, 0.125, ((1, 8),))
    content_weights = bell_draw(key_list[2], (D, H * DK), D ** -0.5, 0.125, ((1, 8),))
    lookup_weights = bell_draw(key_list[3], (D, H * DK), D ** -0.5, 0.125, ((1, 8),))
    forgetting_weights = bell_draw(key_list[4], (D, H), D ** -0.5, 0.125)
    update_intensity_weights = bell_draw(key_list[5], (D, H), D ** -0.5, 0.125)
    forgetting_speeds = draw_forgetting_speeds(jax.random.fold_in(key_list[12], 71), 0)
    update_intensity_ceiling = draw_update_intensity_ceiling(jax.random.fold_in(key_list[12], 71), 0)
    forgetting_multiplier = draw_forgetting_multiplier(jax.random.fold_in(key_list[12], 71), 0)
    spike_offsets = draw_spike_offsets(jax.random.fold_in(key_list[12], 71), 0)
    upcoming_element_vector = bell_draw(key_list[10], (NSEQ, D), 1.0, 6.0, ((0, 2),))
    retrieval_rms_multiplier = jnp.clip(1.0 + 0.18 * jax.random.normal(key_list[11], (DK,), jnp.float32), 0.1, 1.9)
    return dict(prompt_elements=prompt_elements, address_weights=address_weights, content_weights=content_weights, lookup_weights=lookup_weights, forgetting_weights=forgetting_weights, update_intensity_weights=update_intensity_weights, forgetting_speeds=forgetting_speeds, update_intensity_ceiling=update_intensity_ceiling, forgetting_multiplier=forgetting_multiplier, spike_offsets=spike_offsets, upcoming_element_vector=upcoming_element_vector, retrieval_rms_multiplier=retrieval_rms_multiplier)


HIGH = lax.Precision.HIGHEST
EPS = 1e-06

def silu_f(values):
    return values * jax.nn.sigmoid(values)

def unit_rows(values):
    return values * lax.rsqrt(lax.optimization_barrier(jnp.sum(values * values, axis=-1, keepdims=True)) + EPS)

def unit_inverse(lower):
    eye = jnp.eye(lower.shape[-1], dtype=jnp.float32)
    power = -lower
    result = eye + power
    degree = 2
    while degree < lower.shape[-1]:
        power = jnp.matmul(power, power, precision=HIGH)
        result = jnp.matmul(result, eye + power, precision=HIGH)
        degree = degree * 2
    return result

def head_inputs(flat, address_weights, content_weights, decay_cols, strength_cols, forgetting_speeds, update_intensity_ceiling, head_dim):
    count = flat.shape[0]
    key_raw = lax.optimization_barrier(jnp.dot(flat, address_weights, preferred_element_type=jnp.float32).astype(jnp.bfloat16))
    value_raw = lax.optimization_barrier(jnp.dot(flat, content_weights, preferred_element_type=jnp.float32).astype(jnp.bfloat16))
    keys = unit_rows(silu_f(key_raw.astype(jnp.float32)).reshape(count, -1, head_dim))
    values = silu_f(value_raw.astype(jnp.float32)).reshape(count, -1, head_dim)
    decay_pre = jnp.dot(flat, decay_cols, preferred_element_type=jnp.float32)
    strength_pre = jnp.dot(flat, strength_cols, preferred_element_type=jnp.float32)
    speed_addend = -forgetting_speeds * jax.nn.softplus(decay_pre)
    strength = update_intensity_ceiling * jax.nn.sigmoid(strength_pre)
    return (keys, values, speed_addend, strength)

def to_blocks(values, seqs):
    shaped = values.reshape((seqs, -1) + values.shape[1:])
    moved = jnp.moveaxis(shaped, 2, 1)
    return moved.reshape((moved.shape[0] * moved.shape[1], -1, BLK) + moved.shape[3:])

def block_terms(keys, values, forgetting_exponent, strength):
    size = keys.shape[2]
    cumulative = jnp.cumsum(forgetting_exponent, axis=-1)
    places = jnp.arange(size)
    inclusive = places[:, None] >= places[None, :]
    strict = places[:, None] > places[None, :]
    spread = jnp.where(inclusive, cumulative[..., :, None] - cumulative[..., None, :], -jnp.inf)
    weighted = keys * strength[..., None]
    lower = jnp.where(strict, jnp.einsum('gncd,gnmd->gncm', weighted, keys, precision=HIGH) * jnp.exp(spread), 0.0)
    solved = unit_inverse(lower)
    targets = jnp.matmul(solved, values * strength[..., None], precision=HIGH)
    erasers = jnp.matmul(solved, weighted * jnp.exp(cumulative)[..., None], precision=HIGH)
    final_log = cumulative[..., -1]
    faded = keys * jnp.exp(final_log[..., None] - cumulative)[..., None]
    return (targets, erasers, faded, final_log)

def finish(query, keys, values, speed_addend, strength, query_state, key_state, retrieval_rms_multiplier):
    match = lax.optimization_barrier(jnp.sum(query * keys, axis=-1)) * strength
    fading = jnp.exp(speed_addend)
    mixed = fading[..., None] * (query_state - match[..., None] * key_state) + match[..., None] * values
    scaled = mixed * lax.rsqrt(lax.optimization_barrier(jnp.mean(mixed * mixed, axis=-1, keepdims=True)) + EPS) * retrieval_rms_multiplier
    return scaled.reshape(scaled.shape[0], -1).astype(jnp.bfloat16)

def new_query(upcoming_element_vector, lookup_weights, head_dim):
    query_raw = lax.optimization_barrier(jnp.dot(upcoming_element_vector, lookup_weights, preferred_element_type=jnp.float32).astype(jnp.bfloat16))
    query = unit_rows(silu_f(query_raw.astype(jnp.float32)).reshape(upcoming_element_vector.shape[0], -1, head_dim))
    return query * head_dim ** (-0.5)

def reference(prompt_elements, address_weights, content_weights, lookup_weights, forgetting_weights, update_intensity_weights, forgetting_speeds, update_intensity_ceiling, forgetting_multiplier, spike_offsets, upcoming_element_vector, retrieval_rms_multiplier):
    nseq, length, width = prompt_elements.shape
    head_dim = retrieval_rms_multiplier.shape[0]
    attention_group_number = forgetting_speeds.shape[0]
    flat = prompt_elements.reshape(nseq * length, width)
    keys, values, speed_addend, strength = head_inputs(flat, address_weights, content_weights, forgetting_weights, update_intensity_weights, forgetting_speeds, update_intensity_ceiling, head_dim)
    forgetting_exponent = speed_addend * forgetting_multiplier.reshape(-1, attention_group_number) + spike_offsets.reshape(-1, attention_group_number)
    targets, erasers, faded, final_log = block_terms(to_blocks(keys, nseq), to_blocks(values, nseq), to_blocks(forgetting_exponent, nseq), to_blocks(strength, nseq))

    def advance(state, inputs):
        target, eraser, fade, final = inputs
        fresh = target - jnp.matmul(eraser, state, precision=HIGH)
        state = state * jnp.exp(final)[:, None, None] + jnp.matmul(jnp.swapaxes(fade, -1, -2), fresh, precision=HIGH)
        return (state, None)
    moved = tuple((jnp.moveaxis(item, 1, 0) for item in (targets, erasers, faded, final_log)))
    state, _ = lax.scan(advance, jnp.zeros((nseq * attention_group_number, head_dim, head_dim), jnp.float32), moved)
    stored = state.reshape(nseq, attention_group_number, head_dim, head_dim)
    cache = stored.astype(jnp.bfloat16)
    query = new_query(upcoming_element_vector, lookup_weights, head_dim)
    new_keys, new_values, rate_new, strength_new = head_inputs(upcoming_element_vector, address_weights, content_weights, forgetting_weights, update_intensity_weights, forgetting_speeds, update_intensity_ceiling, head_dim)
    query_state = jnp.einsum('shk,shkv->shv', query, stored, precision=HIGH)
    key_state = jnp.einsum('shk,shkv->shv', new_keys, stored, precision=HIGH)
    read = finish(query, new_keys, new_values, rate_new, strength_new, query_state, key_state, retrieval_rms_multiplier)
    return (cache, read)
```

```python
import jax
import jax.numpy as jnp
from jax import lax
from jax.experimental import pallas as pl
from jax.experimental.pallas import tpu as pltpu
from jax.sharding import PartitionSpec as P

EPS = 1e-06
F32 = jnp.float32
BF16 = jnp.bfloat16
MESH = pl.DeviceIdType.MESH
NY = 8
NZ = 4
N = NY * NZ
CH = 128
HD = 128
NN = (((1,), (0,)), ((), ()))
NT = (((1,), (1,)), ((), ()))


def dot1(a, b, dims=NN):
    return lax.dot_general(a.astype(BF16), b.astype(BF16), dims, preferred_element_type=F32)


def halves(a):
    high = a.astype(BF16)
    return high, (a - high.astype(F32)).astype(BF16)


def dot3(a, b):
    ah, al = halves(a)
    bh, bl = halves(b)
    left = jnp.concatenate([ah, ah, al], axis=1)
    right = jnp.concatenate([bh, bl, bh], axis=0)
    return lax.dot_general(left, right, NN, preferred_element_type=F32)


def silu(z):
    return z / (1.0 + jnp.exp(-z))


def softplus(z):
    return jnp.maximum(z, 0.0) + jnp.log1p(jnp.exp(-jnp.abs(z)))


def sigmoid(z):
    return 1.0 / (1.0 + jnp.exp(-z))


def unit_rows(z):
    return z * lax.rsqrt(jnp.sum(z * z, axis=-1, keepdims=True) + EPS)


def iota(shape, dim):
    return lax.broadcasted_iota(jnp.int32, shape, dim)


def compose(early, late_a, late_b):
    moved = dot3(early, late_a)
    return moved[:HD], moved[HD:] + late_b


def chunk_map(k, v, c, beta):
    rows, cols = iota((CH, CH), 0), iota((CH, CH), 1)
    c_cols = jnp.broadcast_to(c, (CH, CH))
    c_rows = jnp.transpose(c_cols)
    end = c[:, CH - 1 :]
    match = dot1(k, k, NT)
    power = jnp.where(cols > rows, match * beta * jnp.exp(c_cols - c_rows), 0.0)
    k_t, v_t = jnp.transpose(k), jnp.transpose(v)
    rhs = jnp.concatenate([k_t * (-beta * jnp.exp(c)), v_t * beta], axis=0)
    both = dot1(jnp.concatenate([rhs, power], axis=0), power)
    rhs = rhs - both[: 2 * HD]
    power = both[2 * HD :]
    for _ in range(5):
        both = dot1(jnp.concatenate([rhs, power], axis=0), power)
        rhs = rhs + both[: 2 * HD]
        power = both[2 * HD :]
    rhs = rhs + dot1(rhs, power)
    faded = k * jnp.exp(end - c_rows)
    out = dot3(rhs, faded)
    return out[:HD] + jnp.where(rows == cols, jnp.exp(end), 0.0), out[HD:]


def kernel(
    x_hbm,
    wk_hbm,
    wv_hbm,
    wq_hbm,
    wf_hbm,
    wu_hbm,
    speed_ref,
    ceil_ref,
    mult_hbm,
    spike_hbm,
    up_hbm,
    gain_hbm,
    cache_ref,
    read_ref,
    xs,
    wkv,
    wqs,
    wfs,
    wus,
    mults,
    spikes,
    ups,
    gains,
    dsc,
    uq,
    uk,
    other_map,
    own_map,
    pair_map,
    row_map,
    row_sum,
    col_map,
    msg,
    fin,
    lsem,
    s1,
    r1,
    s2,
    r2,
    s3,
    r3,
    s4,
    r4,
):
    sp = lax.axis_index("sp")
    tp = lax.axis_index("tp")
    y, z = sp % NY, sp // NY
    core = tp % 2
    par, pair = y % 2, y // 2
    turned = (pair - core + 4) % 4
    s = (par + (turned + 1) // 2) % 2
    other = 1 - s
    vy = (y - 2 * core + NY) % NY
    half = vy % 4 - 1
    is_rx = (vy % 4 == 1) | (vy % 4 == 2)
    head = tp % wf_hbm.shape[0]

    def rx_y(seq, c):
        return ((1 - seq) * 4 + 1 + c + 2 * core) % NY

    loads = [
        pltpu.make_async_copy(wk_hbm, wkv.at[:, 0:HD], lsem.at[0]),
        pltpu.make_async_copy(wv_hbm, wkv.at[:, HD : 2 * HD], lsem.at[1]),
        pltpu.make_async_copy(x_hbm.at[other], xs.at[other], lsem.at[2]),
        pltpu.make_async_copy(wf_hbm, wfs, lsem.at[3]),
        pltpu.make_async_copy(wu_hbm, wus, lsem.at[4]),
        pltpu.make_async_copy(mult_hbm, mults, lsem.at[5]),
        pltpu.make_async_copy(spike_hbm, spikes, lsem.at[6]),
        pltpu.make_async_copy(x_hbm.at[s], xs.at[s], lsem.at[7]),
        pltpu.make_async_copy(wq_hbm, wqs, lsem.at[8]),
        pltpu.make_async_copy(up_hbm, ups, lsem.at[9]),
        pltpu.make_async_copy(gain_hbm, gains, lsem.at[10]),
    ]
    for load in loads:
        load.start()

    barrier = pltpu.get_barrier_semaphore()
    for i in range(1, N):
        pl.semaphore_signal(
            barrier, inc=1, device_id={"sp": (sp + i) % N}, device_id_type=MESH
        )

    speed = speed_ref[0]
    ceiling = ceil_ref[0]
    for i in range(7):
        loads[i].wait()
    w_all = wkv[...]
    wfu = jnp.concatenate([wfs[...].astype(F32), wus[...].astype(F32)], axis=0).astype(BF16)
    heads = wf_hbm.shape[0]

    def seq_map(seq):
        x = xs[seq]
        raw = lax.dot_general(x, w_all, NN, preferred_element_type=F32)
        raw = raw.astype(BF16).astype(F32)
        act = silu(raw)
        k, v = unit_rows(act[:, :HD]), act[:, HD:]
        dsc[...] = lax.dot_general(wfu, x, NT, preferred_element_type=F32)
        decay = dsc[pl.ds(head, 1), :]
        strength = dsc[pl.ds(heads + head, 1), :]
        g = -speed * softplus(decay) * mults[seq] + spikes[seq]
        beta = ceiling * sigmoid(strength)
        g_high = g.astype(BF16).astype(F32)
        g_rest = g - g_high
        g_mid = g_rest.astype(BF16).astype(F32)
        g_low = g_rest - g_mid
        row = iota((8, CH), 0)
        parts = jnp.zeros((8, CH), F32)
        place = 0
        for i in range(2):
            for part in (g_high, g_mid, g_low):
                parts = jnp.where(row == place, part[:, i * CH : (i + 1) * CH], parts)
                place += 1
        upper = jnp.where(iota((CH, CH), 0) <= iota((CH, CH), 1), 1.0, 0.0)
        sums = dot1(parts, upper)
        maps = []
        for i in range(2):
            c = sums[3 * i : 3 * i + 1] + sums[3 * i + 1 : 3 * i + 2] + sums[3 * i + 2 : 3 * i + 3]
            sl = slice(i * CH, (i + 1) * CH)
            maps.append(chunk_map(k[sl], v[sl], c, beta[:, sl]))
        early = jnp.concatenate(maps[0], axis=0)
        return compose(early, maps[1][0], maps[1][1])

    a, b = seq_map(other)
    other_map[0:HD] = a
    other_map[HD : 2 * HD] = b
    pl.semaphore_wait(barrier, N - 1)
    partner = sp + 1 - 2 * par
    swap = pltpu.make_async_remote_copy(
        src_ref=other_map,
        dst_ref=own_map.at[par],
        send_sem=s1,
        recv_sem=r1,
        device_id={"sp": partner},
        device_id_type=MESH,
    )
    swap.start()
    loads[7].wait()
    a, b = seq_map(s)
    own_map[par, 0:HD] = a
    own_map[par, HD : 2 * HD] = b
    pltpu.make_async_remote_copy(
        src_ref=other_map,
        dst_ref=own_map.at[1 - par],
        send_sem=s1,
        recv_sem=r1,
        device_id={"sp": partner},
        device_id_type=MESH,
    ).wait_recv()
    a, b = compose(own_map[0], own_map[1, 0:HD], own_map[1, HD : 2 * HD])
    pair_map[0:HD] = a
    pair_map[HD : 2 * HD] = b

    def row_copies(c, target, slot):
        return [
            pltpu.make_async_remote_copy(
                src_ref=pair_map.at[pl.ds(start, size)],
                dst_ref=row_map.at[slot, pl.ds(place, size)],
                send_sem=s2.at[c, i],
                recv_sem=r2.at[slot, i],
                device_id={"sp": target},
                device_id_type=MESH,
            )
            for i, (start, place, size) in enumerate(((0, 0, HD), (HD + 64 * c, HD, 64)))
        ]

    for c in range(2):
        target = z * NY + rx_y(s, c)

        @pl.when(target != sp)
        def _():
            for copy in row_copies(c, target, pair):
                copy.start()

    for i in range(8, 11):
        loads[i].wait()
    u = ups[...]
    u_raw = lax.dot_general(u, w_all, NN, preferred_element_type=F32).astype(BF16).astype(F32)
    q_raw = lax.dot_general(u, wqs[...], NN, preferred_element_type=F32).astype(BF16).astype(F32)
    u_pre = lax.dot_general(u, wfu, NT, preferred_element_type=F32)
    lane = iota(u_pre.shape, 1)
    u_decay = jnp.sum(jnp.where(lane == head, u_pre, 0.0), axis=1, keepdims=True)
    u_strength = jnp.sum(jnp.where(lane == heads + head, u_pre, 0.0), axis=1, keepdims=True)
    u_act = silu(u_raw)
    new_k, new_v = unit_rows(u_act[:, :HD]), u_act[:, HD:]
    query = unit_rows(silu(q_raw)) * HD ** (-0.5)
    uq[...] = query
    uk[...] = new_k

    @pl.when(is_rx)
    def _():
        row_map[pair, 0:HD] = pair_map[0:HD]
        row_map[pair, HD : HD + 64] = pair_map[pl.ds(HD + 64 * half, 64)]
        for i in range(1, 4):
            for copy in row_copies(0, sp, (pair + i) % 4):
                copy.wait_recv()
        total = row_map[0]
        for i in range(1, 4):
            a, b = compose(total, row_map[i, 0:HD], row_map[i, HD : HD + 64])
            total = jnp.concatenate([a, b], axis=0)
        row_sum[...] = total

        def col_copy(first, size, slot):
            return pltpu.make_async_remote_copy(
                src_ref=row_sum.at[pl.ds(first, size)],
                dst_ref=col_map.at[slot, pl.ds(first, size)],
                send_sem=s3,
                recv_sem=r3.at[slot],
                device_id={"sp": 2 * NY + y},
                device_id_type=MESH,
            )

        @pl.when(z == 0)
        def _():
            col_copy(HD, 64, 0).start()
            col_copy(HD, 64, 0).wait_send()

        @pl.when((z == 1) | (z == 3))
        def _():
            col_copy(0, HD + 64, z).start()
            col_copy(0, HD + 64, z).wait_send()

        @pl.when(z == 2)
        def _():
            q_row, k_row = uq[pl.ds(s, 1), :], uk[pl.ds(s, 1), :]
            at, lanes = iota((8 * N, HD), 0), iota((8 * N, HD), 1)
            inner = at % 8
            picked = jnp.where((inner < 4) & (lanes == 4 * (at // 8) + inner), 1.0, 0.0)
            picked = jnp.where(inner == 4, q_row, picked)
            picked = jnp.where(inner == 5, k_row, picked)
            col_copy(0, HD + 64, 3).wait_recv()
            late_a, late_b = col_map[3, 0:HD], col_map[3, HD : HD + 64]
            a, b = compose(row_sum[...], late_a, late_b)
            col_copy(HD, 64, 0).wait_recv()
            col_copy(0, HD + 64, 1).wait_recv()
            early = dot3(col_map[0, HD : HD + 64], col_map[1, 0:HD]) + col_map[1, HD : HD + 64]
            state = dot3(early, a) + b
            state = jnp.concatenate([state, state], axis=0)
            state = jnp.where(iota((HD, HD), 0) // 64 == half, state, 0.0)
            out = lax.dot_general(
                picked, state, NT, precision=lax.Precision.HIGHEST, preferred_element_type=F32
            )
            msg[...] = out.reshape(N, 8, HD)
            copies = []
            for i in range(1, N):
                to = (sp + i) % N
                copy = pltpu.make_async_remote_copy(
                    src_ref=msg.at[to],
                    dst_ref=fin.at[s, half],
                    send_sem=s4.at[i],
                    recv_sem=r4.at[s, half],
                    device_id={"sp": to},
                    device_id_type=MESH,
                )
                copy.start()
                copies.append(copy)
            fin[s, half] = msg[sp]
            for copy in copies:
                copy.wait_send()

    swap.wait_send()
    for c in range(2):
        target = z * NY + rx_y(s, c)

        @pl.when(target != sp)
        def _():
            for copy in row_copies(c, target, pair):
                copy.wait_send()

    for seq in range(2):
        for c in range(2):

            @pl.when(2 * NY + rx_y(seq, c) != sp)
            def _():
                pltpu.make_async_remote_copy(
                    src_ref=msg.at[0],
                    dst_ref=fin.at[seq, c],
                    send_sem=s4.at[0],
                    recv_sem=r4.at[seq, c],
                    device_id={"sp": sp},
                    device_id_type=MESH,
                ).wait_recv()

    tiles = [fin[seq, 0] + fin[seq, 1] for seq in range(2)]
    for seq in range(2):
        cache_ref[seq, 0] = tiles[seq][0:4].astype(BF16)
    query_state = jnp.concatenate([tile[4:5] for tile in tiles], axis=0)
    key_state = jnp.concatenate([tile[5:6] for tile in tiles], axis=0)
    rate = -speed * softplus(u_decay)
    match = jnp.sum(query * new_k, axis=-1, keepdims=True) * (ceiling * sigmoid(u_strength))
    mixed = jnp.exp(rate) * (query_state - match * key_state) + match * new_v
    scale = lax.rsqrt(jnp.mean(mixed * mixed, axis=-1, keepdims=True) + EPS)
    read_ref[...] = (mixed * scale * gains[...]).astype(BF16)


def on_device(x, wk, wv, wq, wf, wu, speeds, ceilings, mult, spike, up, gain):
    seqs, span, width = x.shape
    heads = wf.shape[1]
    any_space = pl.BlockSpec(memory_space=pl.ANY)
    smem = pl.BlockSpec(memory_space=pltpu.SMEM)
    vmem = pl.BlockSpec(memory_space=pltpu.VMEM)
    dma = pltpu.SemaphoreType.DMA
    return pl.pallas_call(
        kernel,
        out_shape=(
            jax.ShapeDtypeStruct((seqs, 1, HD // N, HD), BF16),
            jax.ShapeDtypeStruct((seqs, HD), BF16),
        ),
        in_specs=[any_space] * 6 + [smem] * 2 + [any_space] * 4,
        out_specs=(vmem, vmem),
        scratch_shapes=[
            pltpu.VMEM((seqs, span, width), BF16),
            pltpu.VMEM((width, 2 * HD), BF16),
            pltpu.VMEM((width, HD), BF16),
            pltpu.VMEM((heads, width), BF16),
            pltpu.VMEM((heads, width), BF16),
            pltpu.VMEM((seqs, 1, span), F32),
            pltpu.VMEM((seqs, 1, span), F32),
            pltpu.VMEM((seqs, width), BF16),
            pltpu.VMEM((1, HD), F32),
            pltpu.VMEM((2 * heads, span), F32),
            pltpu.VMEM((seqs, HD), F32),
            pltpu.VMEM((seqs, HD), F32),
            pltpu.VMEM((2 * HD, HD), F32),
            pltpu.VMEM((2, 2 * HD, HD), F32),
            pltpu.VMEM((2 * HD, HD), F32),
            pltpu.VMEM((4, HD + 64, HD), F32),
            pltpu.VMEM((HD + 64, HD), F32),
            pltpu.VMEM((4, HD + 64, HD), F32),
            pltpu.VMEM((N, 8, HD), F32),
            pltpu.VMEM((2, 2, 8, HD), F32),
            dma((11,)),
            dma,
            dma,
            dma((2, 2)),
            dma((4, 2)),
            dma,
            dma((4,)),
            dma((N,)),
            dma((2, 2)),
        ],
        compiler_params=pltpu.CompilerParams(collective_id=0, has_side_effects=True),
    )(
        x,
        wk,
        wv,
        wq,
        wf.T,
        wu.T,
        speeds,
        ceilings,
        jnp.swapaxes(mult, 1, 2),
        jnp.swapaxes(spike, 1, 2),
        up,
        gain.reshape(1, -1),
    )


def solution(mesh):
    placed = (
        P("gr", "sp", None),
        P(None, "tp"),
        P(None, "tp"),
        P(None, "tp"),
        P(),
        P(),
        P("tp"),
        P("tp"),
        P("gr", "sp", "tp"),
        P("gr", "sp", "tp"),
        P("gr", None),
        P(),
    )
    return jax.shard_map(
        on_device,
        mesh=mesh,
        in_specs=placed,
        out_specs=(P("gr", "tp", "sp", None), P("gr", "tp")),
        check_vma=False,
    )
```

```python
import jax
import jax.numpy as jnp
from jax import lax
from jax.experimental import pallas as pl
from jax.experimental.pallas import tpu as pltpu
from jax.sharding import PartitionSpec as P

EPS = 1e-06
F32 = jnp.float32
BF16 = jnp.bfloat16
MESH = pl.DeviceIdType.MESH
NY = 8
NZ = 4
N = NY * NZ
ZR = 3
RX0, RX1 = 5, 2
FIRST = (0, 1, 7, 2, 6, 3, 5, 4)
OUT = pltpu.VMEM
CH = 128
HD = 128
NN = (((1,), (0,)), ((), ()))
NT = (((1,), (1,)), ((), ()))


def dot1(a, b, dims=NN):
    return lax.dot_general(a.astype(BF16), b.astype(BF16), dims, preferred_element_type=F32)


def halves(a):
    high = a.astype(BF16)
    return high, (a - high.astype(F32)).astype(BF16)


def dot3(a, b):
    ah, al = halves(a)
    bh, bl = halves(b)
    left = jnp.concatenate([ah, ah, al], axis=1)
    right = jnp.concatenate([bh, bl, bh], axis=0)
    return lax.dot_general(left, right, NN, preferred_element_type=F32)


def silu(z):
    return z / (1.0 + jnp.exp(-z))


def softplus(z):
    return jnp.maximum(z, 0.0) + jnp.log1p(jnp.exp(-jnp.abs(z)))


def sigmoid(z):
    return 1.0 / (1.0 + jnp.exp(-z))


def unit_rows(z):
    return z * lax.rsqrt(jnp.sum(z * z, axis=-1, keepdims=True) + EPS)


def iota(shape, dim):
    return lax.broadcasted_iota(jnp.int32, shape, dim)


def compose(early, late_a, late_b):
    moved = dot3(early, late_a)
    return moved[:HD], moved[HD:] + late_b


def chunk_map(k, v, c, beta):
    rows, cols = iota((CH, CH), 0), iota((CH, CH), 1)
    c_cols = jnp.broadcast_to(c, (CH, CH))
    c_rows = jnp.transpose(c_cols)
    end = c[:, CH - 1 :]
    match = dot1(k, k, NT)
    power = jnp.where(cols > rows, match * beta * jnp.exp(c_cols - c_rows), 0.0)
    k_t, v_t = jnp.transpose(k), jnp.transpose(v)
    rhs = jnp.concatenate([k_t * (-beta * jnp.exp(c)), v_t * beta], axis=0)
    both = dot1(jnp.concatenate([rhs, power], axis=0), power)
    rhs = rhs - both[: 2 * HD]
    power = both[2 * HD :]
    for _ in range(5):
        both = dot1(jnp.concatenate([rhs, power], axis=0), power)
        rhs = rhs + both[: 2 * HD]
        power = both[2 * HD :]
    rhs = rhs + dot1(rhs, power)
    faded = k * jnp.exp(end - c_rows)
    out = dot3(rhs, faded)
    return out[:HD] + jnp.where(rows == cols, jnp.exp(end), 0.0), out[HD:]


def kernel(
    x_hbm,
    wk_hbm,
    wv_hbm,
    wq_hbm,
    wf_hbm,
    wu_hbm,
    speed_ref,
    ceil_ref,
    mult_hbm,
    spike_hbm,
    up_hbm,
    gain_hbm,
    out_ref,
    xs,
    wkv,
    wqs,
    wfs,
    wus,
    mults,
    spikes,
    ups,
    gains,
    dsc,
    uq,
    uk,
    other_map,
    own_map,
    pair_map,
    row_map,
    row_sum,
    col_map,
    msg,
    fin,
    lsem,
    s1,
    r1,
    s2,
    r2,
    s3,
    r3,
    s4,
    r4,
):
    sp = lax.axis_index("sp")
    tp = lax.axis_index("tp")
    y, z = sp % NY, sp // NY
    core = tp % 2
    par, pair = y % 2, y // 2
    turned = (pair - core + 4) % 4
    s = (par + (turned + 1) // 2) % 2
    other = 1 - s

    def rx_y(seq):
        return (RX0 + (RX1 - RX0) * seq + 2 * core) % NY

    is_rx = y == rx_y(s)
    head = tp % wf_hbm.shape[0]

    pairs = [
        (wk_hbm, wkv.at[:, 0:HD]),
        (wv_hbm, wkv.at[:, HD : 2 * HD]),
        (x_hbm.at[other], xs.at[other]),
        (wf_hbm, wfs),
        (wu_hbm, wus),
        (mult_hbm, mults),
        (spike_hbm, spikes),
        (x_hbm.at[s], xs.at[s]),
        (wq_hbm, wqs),
        (up_hbm, ups),
        (gain_hbm, gains),
    ]
    loads = [pltpu.make_async_copy(a, b, lsem.at[i]) for i, (a, b) in enumerate(pairs)]
    first = 7
    for load in loads[:first]:
        load.start()

    barrier = pltpu.get_barrier_semaphore()

    def greet(device):
        pl.semaphore_signal(barrier, inc=1, device_id={"sp": device}, device_id_type=MESH)

    partner = sp + 1 - 2 * par
    greet(partner)

    @pl.when(is_rx)
    def _():
        for i in range(1, 4):
            there = (pair + i) % 4
            greet(z * NY + 2 * there + (s + ((there - core + 4) % 4 + 1) // 2) % 2)

        @pl.when(z == ZR)
        def _():
            for i in range(NZ):
                if i != ZR:
                    greet(i * NY + y)

    with jax.named_scope("p_load"):
        for load in loads[:first]:
            load.wait()
        for load in loads[first:]:
            load.start()
        speed, ceiling = speed_ref[0], ceil_ref[0]
    w_all = wkv[...]
    wfu = jnp.concatenate([wfs[...].astype(F32), wus[...].astype(F32)], axis=0).astype(BF16)
    heads = wf_hbm.shape[0]

    def seq_map(seq):
        x = xs[seq]
        raw = lax.dot_general(x, w_all, NN, preferred_element_type=F32)
        raw = raw.astype(BF16).astype(F32)
        act = silu(raw)
        k, v = unit_rows(act[:, :HD]), act[:, HD:]
        dsc[...] = lax.dot_general(wfu, x, NT, preferred_element_type=F32)
        decay = dsc[pl.ds(head, 1), :]
        strength = dsc[pl.ds(heads + head, 1), :]
        g = -speed * softplus(decay) * mults[seq] + spikes[seq]
        beta = ceiling * sigmoid(strength)
        g_high = g.astype(BF16).astype(F32)
        g_rest = g - g_high
        g_mid = g_rest.astype(BF16).astype(F32)
        g_low = g_rest - g_mid
        row = iota((8, CH), 0)
        parts = jnp.zeros((8, CH), F32)
        place = 0
        for i in range(2):
            for part in (g_high, g_mid, g_low):
                parts = jnp.where(row == place, part[:, i * CH : (i + 1) * CH], parts)
                place += 1
        upper = jnp.where(iota((CH, CH), 0) <= iota((CH, CH), 1), 1.0, 0.0)
        sums = dot1(parts, upper)
        maps = []
        for i in range(2):
            c = sums[3 * i : 3 * i + 1] + sums[3 * i + 1 : 3 * i + 2] + sums[3 * i + 2 : 3 * i + 3]
            sl = slice(i * CH, (i + 1) * CH)
            maps.append(chunk_map(k[sl], v[sl], c, beta[:, sl]))
        early = jnp.concatenate(maps[0], axis=0)
        return compose(early, maps[1][0], maps[1][1])

    with jax.named_scope("p_seqA"):
        a, b = seq_map(other)
        other_map[0:HD] = a
        other_map[HD : 2 * HD] = b
    with jax.named_scope("p_barrier"):
        pl.semaphore_wait(barrier, jnp.where(is_rx & (z == ZR), 1, 2))
    swap = pltpu.make_async_remote_copy(
        src_ref=other_map,
        dst_ref=own_map.at[par],
        send_sem=s1,
        recv_sem=r1,
        device_id={"sp": partner},
        device_id_type=MESH,
    )
    swap.start()
    with jax.named_scope("p_seqB"):
        loads[first].wait()
        a, b = seq_map(s)
        own_map[par, 0:HD] = a
        own_map[par, HD : 2 * HD] = b
    with jax.named_scope("p_r1wait"):
        pltpu.make_async_remote_copy(
            src_ref=other_map,
            dst_ref=own_map.at[1 - par],
            send_sem=s1,
            recv_sem=r1,
            device_id={"sp": partner},
            device_id_type=MESH,
        ).wait_recv()
    with jax.named_scope("p_pair"):
        a, b = compose(own_map[0], own_map[1, 0:HD], own_map[1, HD : 2 * HD])
        pair_map[0:HD] = a
        pair_map[HD : 2 * HD] = b
    def row_copy(slot):
        return pltpu.make_async_remote_copy(
            src_ref=pair_map,
            dst_ref=row_map.at[slot],
            send_sem=s2,
            recv_sem=r2.at[slot],
            device_id={"sp": z * NY + rx_y(s)},
            device_id_type=MESH,
        )

    @pl.when(jnp.logical_not(is_rx))
    def _():
        row_copy(pair).start()

    with jax.named_scope("p_up"):
        for load in loads[first + 1 :]:
            load.wait()
        u = ups[...]
        u_raw = lax.dot_general(u, w_all, NN, preferred_element_type=F32).astype(BF16).astype(F32)
        q_raw = lax.dot_general(u, wqs[...], NN, preferred_element_type=F32).astype(BF16).astype(F32)
        u_pre = lax.dot_general(u, wfu, NT, preferred_element_type=F32)
        lane = iota(u_pre.shape, 1)
        u_decay = jnp.sum(jnp.where(lane == head, u_pre, 0.0), axis=1, keepdims=True)
        u_strength = jnp.sum(jnp.where(lane == heads + head, u_pre, 0.0), axis=1, keepdims=True)
        u_act = silu(u_raw)
        new_k, new_v = unit_rows(u_act[:, :HD]), u_act[:, HD:]
        query = unit_rows(silu(q_raw)) * HD ** (-0.5)
        uq[...] = query
        uk[...] = new_k
    @pl.when(is_rx)
    def _():
        row_map[pair] = pair_map[...]
        with jax.named_scope("p_r2wait"):
            for i in range(1, 4):
                row_copy((pair + i) % 4).wait_recv()
        with jax.named_scope("p_rowsum"):
            a, b = compose(row_map[2], row_map[3, 0:HD], row_map[3, HD:])
            c, d = compose(row_map[0], row_map[1, 0:HD], row_map[1, HD:])
            a, b = compose(jnp.concatenate([c, d], axis=0), a, b)
            row_sum[0:HD] = a
            row_sum[HD:] = b

        def col_copy(first, size, slot):
            return pltpu.make_async_remote_copy(
                src_ref=row_sum.at[pl.ds(first, size)],
                dst_ref=col_map.at[slot, pl.ds(first, size)],
                send_sem=s3,
                recv_sem=r3.at[slot],
                device_id={"sp": ZR * NY + y},
                device_id_type=MESH,
            )

        @pl.when(z == 0)
        def _():
            col_copy(HD, HD, 0).start()
            col_copy(HD, HD, 0).wait_send()

        @pl.when((z != 0) & (z != ZR))
        def _():
            col_copy(0, 2 * HD, z).start()
            col_copy(0, 2 * HD, z).wait_send()

        @pl.when(z == ZR)
        def _():
            q_row, k_row = uq[pl.ds(s, 1), :], uk[pl.ds(s, 1), :]
            at, lanes = iota((8 * N, HD), 0), iota((8 * N, HD), 1)
            inner = at % 8
            picked = jnp.where((inner < 4) & (lanes == 4 * (at // 8) + inner), 1.0, 0.0)
            picked = jnp.where(inner == 4, q_row, picked)
            picked = jnp.where(inner == 5, k_row, picked)
            col_map[ZR] = row_sum[...]
            with jax.named_scope("p_r3wait01"):
                col_copy(HD, HD, 0).wait_recv()
                col_copy(0, 2 * HD, 1).wait_recv()
            with jax.named_scope("p_state1"):
                state = dot3(col_map[0, HD:], col_map[1, 0:HD]) + col_map[1, HD:]
            with jax.named_scope("p_r3wait3"):
                col_copy(0, 2 * HD, 5 - ZR).wait_recv()
            with jax.named_scope("p_state"):
                for i in (2, 3):
                    state = dot3(state, col_map[i, 0:HD]) + col_map[i, HD:]
                out = lax.dot_general(
                    picked, state, NT, precision=lax.Precision.HIGHEST, preferred_element_type=F32
                )
                msg[...] = out.reshape(N, 8, HD)
            def send(to):
                return pltpu.make_async_remote_copy(
                    src_ref=msg.at[to],
                    dst_ref=fin.at[s],
                    send_sem=s4.at[to],
                    recv_sem=r4.at[s],
                    device_id={"sp": to},
                    device_id_type=MESH,
                )

            with jax.named_scope("p_r4send"):
                targets = [i * NY + j for i in range(NZ) for j in FIRST]
                for to in targets:
                    if to // NY == ZR:
                        pl.when(to != sp)(send(to).start)
                    else:
                        send(to).start()
                fin[s] = msg[sp]
            for to in targets:
                if to // NY == ZR:
                    pl.when(to != sp)(send(to).wait_send)
                else:
                    send(to).wait_send()

    swap.wait_send()

    @pl.when(jnp.logical_not(is_rx))
    def _():
        row_copy(pair).wait_send()

    with jax.named_scope("p_r4wait"):
        for seq in range(2):

            @pl.when(ZR * NY + rx_y(seq) != sp)
            def _():
                pltpu.make_async_remote_copy(
                    src_ref=msg.at[0],
                    dst_ref=fin.at[seq],
                    send_sem=s4.at[0],
                    recv_sem=r4.at[seq],
                    device_id={"sp": sp},
                    device_id_type=MESH,
                ).wait_recv()

    with jax.named_scope("p_finish"):
        tiles = [fin[seq] for seq in range(2)]
        query_state = jnp.concatenate([tile[4:5] for tile in tiles], axis=0)
        key_state = jnp.concatenate([tile[5:6] for tile in tiles], axis=0)
        rate = -speed * softplus(u_decay)
        match = jnp.sum(query * new_k, axis=-1, keepdims=True) * (ceiling * sigmoid(u_strength))
        mixed = jnp.exp(rate) * (query_state - match * key_state) + match * new_v
        scale = lax.rsqrt(jnp.mean(mixed * mixed, axis=-1, keepdims=True) + EPS)
        read = mixed * scale * gains[...]
        row = iota((8, HD), 0)
        for seq in range(2):
            out_ref[seq] = jnp.where(row == 4, read[seq : seq + 1], tiles[seq])


def place_outputs(tiles_ref, cache_ref, read_ref):
    for seq in range(2):
        cache_ref[seq, 0] = tiles_ref[seq, 0:4].astype(BF16)
    rows = [tiles_ref[seq, 4:5] for seq in range(2)]
    read_ref[...] = jnp.concatenate(rows, axis=0).astype(BF16)


def on_device(x, wk, wv, wq, wf, wu, speeds, ceilings, mult, spike, up, gain):
    seqs, span, width = x.shape
    heads = wf.shape[1]
    any_space = pl.BlockSpec(memory_space=pl.ANY)
    smem = pl.BlockSpec(memory_space=pltpu.SMEM)
    vmem = pl.BlockSpec(memory_space=pltpu.VMEM)
    dma = pltpu.SemaphoreType.DMA
    out = pl.pallas_call(
        kernel,
        out_shape=OUT((seqs, 8, HD), F32),
        in_specs=[any_space] * 6 + [smem] * 2 + [any_space] * 4,
        out_specs=vmem,
        scratch_shapes=[
            pltpu.VMEM((seqs, span, width), BF16),
            pltpu.VMEM((width, 2 * HD), BF16),
            pltpu.VMEM((width, HD), BF16),
            pltpu.VMEM((heads, width), BF16),
            pltpu.VMEM((heads, width), BF16),
            pltpu.VMEM((seqs, 1, span), F32),
            pltpu.VMEM((seqs, 1, span), F32),
            pltpu.VMEM((seqs, width), BF16),
            pltpu.VMEM((1, HD), F32),
            pltpu.VMEM((2 * heads, span), F32),
            pltpu.VMEM((seqs, HD), F32),
            pltpu.VMEM((seqs, HD), F32),
            pltpu.VMEM((2 * HD, HD), F32),
            pltpu.VMEM((2, 2 * HD, HD), F32),
            pltpu.VMEM((2 * HD, HD), F32),
            pltpu.VMEM((4, 2 * HD, HD), F32),
            pltpu.VMEM((2 * HD, HD), F32),
            pltpu.VMEM((4, 2 * HD, HD), F32),
            pltpu.VMEM((N, 8, HD), F32),
            pltpu.VMEM((2, 8, HD), F32),
            dma((11,)),
            dma,
            dma,
            dma,
            dma((4,)),
            dma,
            dma((4,)),
            dma((N,)),
            dma((2,)),
        ],
        compiler_params=pltpu.CompilerParams(collective_id=0, has_side_effects=True),
    )(
        x,
        wk,
        wv,
        wq,
        wf.T,
        wu.T,
        speeds,
        ceilings,
        jnp.swapaxes(mult, 1, 2),
        jnp.swapaxes(spike, 1, 2),
        up,
        gain.reshape(1, -1),
    )
    return pl.pallas_call(
        place_outputs,
        out_shape=(
            jax.ShapeDtypeStruct((seqs, 1, HD // N, HD), BF16),
            jax.ShapeDtypeStruct((seqs, HD), BF16),
        ),
        in_specs=[vmem],
        out_specs=(vmem, vmem),
    )(pltpu.with_memory_space_constraint(out, pltpu.VMEM))


def solution(mesh):
    placed = (
        P("gr", "sp", None),
        P(None, "tp"),
        P(None, "tp"),
        P(None, "tp"),
        P(),
        P(),
        P("tp"),
        P("tp"),
        P("gr", "sp", "tp"),
        P("gr", "sp", "tp"),
        P("gr", None),
        P(),
    )
    return jax.shard_map(
        on_device,
        mesh=mesh,
        in_specs=placed,
        out_specs=(P("gr", "tp", "sp", None), P("gr", "tp")),
        check_vma=False,
    )
```

```python
import jax
import jax.numpy as jnp
from jax import lax
from jax.experimental import pallas as pl
from jax.experimental.pallas import tpu as pltpu
from jax.sharding import PartitionSpec as P

EPS = 1e-06
F32 = jnp.float32
BF16 = jnp.bfloat16
MESH = pl.DeviceIdType.MESH
NY = 8
NZ = 4
N = NY * NZ
ZR = 3
NK = 4
EARLY = 0
RX0, RX1 = 5, 2
FIRST = (0, 1, 7, 2, 6, 3, 5, 4)
OUT = pltpu.VMEM
CH = 128
HD = 128
NN = (((1,), (0,)), ((), ()))
NT = (((1,), (1,)), ((), ()))


def dot1(a, b, dims=NN):
    return lax.dot_general(a.astype(BF16), b.astype(BF16), dims, preferred_element_type=F32)


def halves(a):
    high = a.astype(BF16)
    return high, (a - high.astype(F32)).astype(BF16)


def dot3(a, b):
    ah, al = halves(a)
    bh, bl = halves(b)
    left = jnp.concatenate([ah, ah, al], axis=1)
    right = jnp.concatenate([bh, bl, bh], axis=0)
    return lax.dot_general(left, right, NN, preferred_element_type=F32)


def silu(z):
    return z / (1.0 + jnp.exp(-z))


def softplus(z):
    return jnp.maximum(z, 0.0) + jnp.log1p(jnp.exp(-jnp.abs(z)))


def sigmoid(z):
    return 1.0 / (1.0 + jnp.exp(-z))


def unit_rows(z):
    return z * lax.rsqrt(jnp.sum(z * z, axis=-1, keepdims=True) + EPS)


def iota(shape, dim):
    return lax.broadcasted_iota(jnp.int32, shape, dim)


def compose(early, late_a, late_b):
    moved = dot3(early, late_a)
    return moved[:HD], moved[HD:] + late_b


def chunk_maps(keys, values, sums, betas):
    some = range(len(keys))
    rows, cols = iota((CH, CH), 0), iota((CH, CH), 1)
    c_rows = [jnp.transpose(jnp.broadcast_to(c, (CH, CH))) for c in sums]
    ends = [c[:, CH - 1 :] for c in sums]
    match = [dot1(k, k, NT) for k in keys]
    k_t = [jnp.transpose(k) for k in keys]
    v_t = [jnp.transpose(v) for v in values]
    power = [
        jnp.where(cols > rows, match[i] * betas[i] * jnp.exp(sums[i] - c_rows[i]), 0.0)
        for i in some
    ]
    rhs = [
        jnp.concatenate([k_t[i] * (-betas[i] * jnp.exp(sums[i])), v_t[i] * betas[i]], axis=0)
        for i in some
    ]
    for level in range(6):
        both = [dot1(jnp.concatenate([power[i], rhs[i]], axis=0), power[i]) for i in some]
        power = [both[i][:CH] for i in some]
        applied = [both[i][CH:] for i in some]
        rhs = [rhs[i] - applied[i] if level == 0 else rhs[i] + applied[i] for i in some]
    rhs = [rhs[i] + dot1(rhs[i], power[i]) for i in some]
    faded = [keys[i] * jnp.exp(ends[i] - c_rows[i]) for i in some]
    out = [dot3(rhs[i], faded[i]) for i in some]
    decayed = [jnp.where(rows == cols, jnp.exp(ends[i]), 0.0) for i in some]
    return [(out[i][:HD] + decayed[i], out[i][HD:]) for i in some]


def kernel(
    x_hbm,
    wk_hbm,
    wv_hbm,
    wq_hbm,
    wf_hbm,
    wu_hbm,
    speed_ref,
    ceil_ref,
    mult_hbm,
    spike_hbm,
    up_hbm,
    gain_hbm,
    out_ref,
    xs,
    wkv,
    wqs,
    wfs,
    wus,
    mults,
    spikes,
    ups,
    gains,
    dsc,
    uq,
    uk,
    other_map,
    own_map,
    pair_map,
    row_map,
    row_sum,
    col_map,
    msg,
    fin,
    lsem,
    s1,
    r1,
    s2,
    r2,
    s3,
    r3,
    s4,
    r4,
    row_ready,
    col_ready,
):
    sp = lax.axis_index("sp")
    tp = lax.axis_index("tp")
    y, z = lax.rem(sp, NY), lax.div(sp, NY)
    core = lax.rem(tp, 2)
    par, pair = lax.rem(y, 2), lax.div(y, 2)

    def offset(there):
        return lax.div(lax.rem(there - core + 4, 4) + 1, 2)

    s = lax.rem(par + offset(pair), 2)
    other = 1 - s

    def rx_y(seq):
        return lax.rem(RX0 + (RX1 - RX0) * seq + 2 * core, NY)

    is_rx = y == rx_y(s)
    heads = wf_hbm.shape[0]
    head = lax.rem(tp, heads)

    depth = wk_hbm.shape[0] // NK
    pieces = [pl.ds(i * depth, depth) for i in range(NK)]
    pairs = [(wf_hbm, wfs), (wu_hbm, wus)]
    for piece in pieces:
        pairs += [
            (wk_hbm.at[piece], wkv.at[piece, 0:HD]),
            (wv_hbm.at[piece], wkv.at[piece, HD : 2 * HD]),
            (x_hbm.at[other, :, piece], xs.at[other, :, piece]),
        ]
    pairs += [
        (mult_hbm, mults),
        (spike_hbm, spikes),
        (x_hbm.at[s], xs.at[s]),
        (wq_hbm, wqs),
        (up_hbm, ups),
        (gain_hbm, gains),
    ]
    loads = [pltpu.make_async_copy(a, b, lsem.at[i]) for i, (a, b) in enumerate(pairs)]
    first = 3 * NK + 4
    for load in loads[:first]:
        load.start()

    barrier = pltpu.get_barrier_semaphore()

    def greet(device):
        pl.semaphore_signal(barrier, inc=1, device_id={"sp": device}, device_id_type=MESH)

    partner = sp + 1 - 2 * par
    greet(partner)

    def senders(signal):
        for i in range(1, 4):
            there = lax.rem(pair + i, 4)
            signal(z * NY + 2 * there + lax.rem(s + offset(there), 2))

    @pl.when(is_rx)
    def _():
        @pl.when(z != ZR)
        def _():
            greet(ZR * NY + y)

    @pl.when(jnp.logical_not(is_rx))
    def _():
        greet(z * NY + rx_y(s))

    speed, ceiling = speed_ref[0], ceil_ref[0]
    loads[0].wait()
    loads[1].wait()
    wfu = jnp.concatenate([wfs[...].astype(F32), wus[...].astype(F32)], axis=0).astype(BF16)

    def project(seq, piece):
        x = xs[seq, :, piece]
        raw = lax.dot_general(x, wkv[piece], NN, preferred_element_type=F32)
        pre = lax.dot_general(wfu[:, piece], x, NT, preferred_element_type=F32)
        return raw, pre

    def seq_map(seq, raw, pre):
        dsc[...] = pre
        raw = raw.astype(BF16).astype(F32)
        act = silu(raw)
        k, v = unit_rows(act[:, :HD]), act[:, HD:]
        decay = dsc[pl.ds(head, 1), :]
        strength = dsc[pl.ds(heads + head, 1), :]
        g = -speed * softplus(decay) * mults[seq] + spikes[seq]
        beta = ceiling * sigmoid(strength)
        g_high = g.astype(BF16).astype(F32)
        g_rest = g - g_high
        g_mid = g_rest.astype(BF16).astype(F32)
        g_low = g_rest - g_mid
        row = iota((8, CH), 0)
        parts = jnp.zeros((8, CH), F32)
        place = 0
        for i in range(2):
            for part in (g_high, g_mid, g_low):
                parts = jnp.where(row == place, part[:, i * CH : (i + 1) * CH], parts)
                place += 1
        upper = jnp.where(iota((CH, CH), 0) <= iota((CH, CH), 1), 1.0, 0.0)
        sums = dot1(parts, upper)
        slices = [slice(i * CH, (i + 1) * CH) for i in range(2)]
        maps = chunk_maps(
            [k[sl] for sl in slices],
            [v[sl] for sl in slices],
            [sums[3 * i : 3 * i + 1] + sums[3 * i + 1 : 3 * i + 2] + sums[3 * i + 2 : 3 * i + 3] for i in range(2)],
            [beta[:, sl] for sl in slices],
        )
        early = jnp.concatenate(maps[0], axis=0)
        return compose(early, maps[1][0], maps[1][1])

    with jax.named_scope("p_seqA"):
        raw, pre = None, None
        for i in range(NK):
            for load in loads[2 + 3 * i : 5 + 3 * i]:
                load.wait()
            if i == NK - 2:
                loads[first].start()
            raw_part, pre_part = project(other, slice(i * depth, (i + 1) * depth))
            raw = raw_part if raw is None else raw + raw_part
            pre = pre_part if pre is None else pre + pre_part
        for load in loads[first + 1 :]:
            load.start()
        for load in loads[first - 2 : first]:
            load.wait()
        a, b = seq_map(other, raw, pre)
        other_map[0:HD] = a
        other_map[HD : 2 * HD] = b
    with jax.named_scope("p_barrier"):
        expected = jnp.where(is_rx, jnp.where(z == ZR, 4 + NZ - 1, 4), 1)
        pl.semaphore_wait(barrier, expected)

    @pl.when(is_rx)
    def _():
        def ready(device):
            pl.semaphore_signal(row_ready, inc=1, device_id={"sp": device}, device_id_type=MESH)

        senders(ready)

        @pl.when(z == ZR)
        def _():
            for i in range(NZ):
                if i != ZR:
                    pl.semaphore_signal(
                        col_ready, inc=1, device_id={"sp": i * NY + y}, device_id_type=MESH
                    )

    swap = pltpu.make_async_remote_copy(
        src_ref=other_map,
        dst_ref=own_map.at[par],
        send_sem=s1,
        recv_sem=r1,
        device_id={"sp": partner},
        device_id_type=MESH,
    )
    early = core == EARLY
    pl.when(early)(swap.start)
    with jax.named_scope("p_seqB"):
        loads[first].wait()
        a, b = seq_map(s, *project(s, slice(0, NK * depth)))
        own_map[par, 0:HD] = a
        own_map[par, HD : 2 * HD] = b
    pl.when(jnp.logical_not(early))(swap.start)
    with jax.named_scope("p_r1wait"):
        pltpu.make_async_remote_copy(
            src_ref=other_map,
            dst_ref=own_map.at[1 - par],
            send_sem=s1,
            recv_sem=r1,
            device_id={"sp": partner},
            device_id_type=MESH,
        ).wait_recv()
    with jax.named_scope("p_pair"):
        a, b = compose(own_map[0], own_map[1, 0:HD], own_map[1, HD : 2 * HD])
        pair_map[0:HD] = a
        pair_map[HD : 2 * HD] = b
    def row_copy(slot):
        return pltpu.make_async_remote_copy(
            src_ref=pair_map,
            dst_ref=row_map.at[slot],
            send_sem=s2,
            recv_sem=r2.at[slot],
            device_id={"sp": z * NY + rx_y(s)},
            device_id_type=MESH,
        )

    @pl.when(jnp.logical_not(is_rx))
    def _():
        pl.semaphore_wait(row_ready, 1)
        row_copy(pair).start()

    with jax.named_scope("p_up"):
        for load in loads[first + 1 :]:
            load.wait()
        w_all = wkv[...]
        u = ups[...]
        u_raw = lax.dot_general(u, w_all, NN, preferred_element_type=F32).astype(BF16).astype(F32)
        q_raw = lax.dot_general(u, wqs[...], NN, preferred_element_type=F32).astype(BF16).astype(F32)
        u_pre = lax.dot_general(u, wfu, NT, preferred_element_type=F32)
        lane = iota(u_pre.shape, 1)
        u_decay = jnp.sum(jnp.where(lane == head, u_pre, 0.0), axis=1, keepdims=True)
        u_strength = jnp.sum(jnp.where(lane == heads + head, u_pre, 0.0), axis=1, keepdims=True)
        u_act = silu(u_raw)
        new_k, new_v = unit_rows(u_act[:, :HD]), u_act[:, HD:]
        query = unit_rows(silu(q_raw)) * HD ** (-0.5)
        uq[...] = query
        uk[...] = new_k
    @pl.when(is_rx)
    def _():
        row_map[pair] = pair_map[...]
        with jax.named_scope("p_r2wait"):
            for i in range(1, 4):
                row_copy(lax.rem(pair + i, 4)).wait_recv()
        with jax.named_scope("p_rowsum"):
            a, b = compose(row_map[2], row_map[3, 0:HD], row_map[3, HD:])
            c, d = compose(row_map[0], row_map[1, 0:HD], row_map[1, HD:])
            a, b = compose(jnp.concatenate([c, d], axis=0), a, b)
            row_sum[0:HD] = a
            row_sum[HD:] = b

        def col_copy(first, size, slot):
            return pltpu.make_async_remote_copy(
                src_ref=row_sum.at[pl.ds(first, size)],
                dst_ref=col_map.at[slot, pl.ds(first, size)],
                send_sem=s3,
                recv_sem=r3.at[slot],
                device_id={"sp": ZR * NY + y},
                device_id_type=MESH,
            )

        @pl.when(z == 0)
        def _():
            pl.semaphore_wait(col_ready, 1)
            col_copy(HD, HD, 0).start()
            col_copy(HD, HD, 0).wait_send()

        @pl.when((z != 0) & (z != ZR))
        def _():
            pl.semaphore_wait(col_ready, 1)
            col_copy(0, 2 * HD, z).start()
            col_copy(0, 2 * HD, z).wait_send()

        @pl.when(z == ZR)
        def _():
            q_row, k_row = uq[pl.ds(s, 1), :], uk[pl.ds(s, 1), :]
            at, lanes = iota((8 * N, HD), 0), iota((8 * N, HD), 1)
            inner = at % 8
            picked = jnp.where((inner < 4) & (lanes == 4 * (at // 8) + inner), 1.0, 0.0)
            picked = jnp.where(inner == 4, q_row, picked)
            picked = jnp.where(inner == 5, k_row, picked)
            col_map[ZR] = row_sum[...]
            with jax.named_scope("p_r3wait01"):
                col_copy(HD, HD, 0).wait_recv()
                col_copy(0, 2 * HD, 1).wait_recv()
            with jax.named_scope("p_state1"):
                state = dot3(col_map[0, HD:], col_map[1, 0:HD]) + col_map[1, HD:]
            with jax.named_scope("p_r3wait3"):
                col_copy(0, 2 * HD, 5 - ZR).wait_recv()
            with jax.named_scope("p_state"):
                for i in (2, 3):
                    state = dot3(state, col_map[i, 0:HD]) + col_map[i, HD:]
                out = lax.dot_general(
                    picked, state, NT, precision=lax.Precision.HIGHEST, preferred_element_type=F32
                )
                msg[...] = out.reshape(N, 8, HD)
            def send(to):
                return pltpu.make_async_remote_copy(
                    src_ref=msg.at[to],
                    dst_ref=fin.at[s],
                    send_sem=s4.at[to],
                    recv_sem=r4.at[s],
                    device_id={"sp": to},
                    device_id_type=MESH,
                )

            with jax.named_scope("p_r4send"):
                targets = [i * NY + j for i in range(NZ) for j in FIRST]
                for to in targets:
                    if to // NY == ZR:
                        pl.when(to != sp)(send(to).start)
                    else:
                        send(to).start()
                fin[s] = msg[sp]
            for to in targets:
                if to // NY == ZR:
                    pl.when(to != sp)(send(to).wait_send)
                else:
                    send(to).wait_send()

    swap.wait_send()

    @pl.when(jnp.logical_not(is_rx))
    def _():
        row_copy(pair).wait_send()

    with jax.named_scope("p_r4wait"):
        for seq in range(2):

            @pl.when(ZR * NY + rx_y(seq) != sp)
            def _():
                pltpu.make_async_remote_copy(
                    src_ref=msg.at[0],
                    dst_ref=fin.at[seq],
                    send_sem=s4.at[0],
                    recv_sem=r4.at[seq],
                    device_id={"sp": sp},
                    device_id_type=MESH,
                ).wait_recv()

    with jax.named_scope("p_finish"):
        tiles = [fin[seq] for seq in range(2)]
        query_state = jnp.concatenate([tile[4:5] for tile in tiles], axis=0)
        key_state = jnp.concatenate([tile[5:6] for tile in tiles], axis=0)
        rate = -speed * softplus(u_decay)
        match = jnp.sum(query * new_k, axis=-1, keepdims=True) * (ceiling * sigmoid(u_strength))
        mixed = jnp.exp(rate) * (query_state - match * key_state) + match * new_v
        scale = lax.rsqrt(jnp.mean(mixed * mixed, axis=-1, keepdims=True) + EPS)
        read = mixed * scale * gains[...]
        row = iota((8, HD), 0)
        for seq in range(2):
            out_ref[seq] = jnp.where(row == 4, read[seq : seq + 1], tiles[seq])


def near(a):
    return pltpu.with_memory_space_constraint(a, pltpu.VMEM)


def place_outputs(tiles_ref, cache_ref, read_ref):
    for seq in range(2):
        cache_ref[seq, 0] = tiles_ref[seq, 0:4].astype(BF16)
    rows = [tiles_ref[seq, 4:5] for seq in range(2)]
    read_ref[...] = jnp.concatenate(rows, axis=0).astype(BF16)


def on_device(x, wk, wv, wq, wf, wu, speeds, ceilings, mult, spike, up, gain):
    seqs, span, width = x.shape
    heads = wf.shape[1]
    any_space = pl.BlockSpec(memory_space=pl.ANY)
    smem = pl.BlockSpec(memory_space=pltpu.SMEM)
    vmem = pl.BlockSpec(memory_space=pltpu.VMEM)
    dma = pltpu.SemaphoreType.DMA
    out = pl.pallas_call(
        kernel,
        out_shape=OUT((seqs, 8, HD), F32),
        in_specs=[any_space] * 6 + [smem] * 2 + [any_space] * 4,
        out_specs=vmem,
        scratch_shapes=[
            pltpu.VMEM((seqs, span, width), BF16),
            pltpu.VMEM((width, 2 * HD), BF16),
            pltpu.VMEM((width, HD), BF16),
            pltpu.VMEM((heads, width), BF16),
            pltpu.VMEM((heads, width), BF16),
            pltpu.VMEM((seqs, 1, span), F32),
            pltpu.VMEM((seqs, 1, span), F32),
            pltpu.VMEM((seqs, width), BF16),
            pltpu.VMEM((1, HD), F32),
            pltpu.VMEM((2 * heads, span), F32),
            pltpu.VMEM((seqs, HD), F32),
            pltpu.VMEM((seqs, HD), F32),
            pltpu.VMEM((2 * HD, HD), F32),
            pltpu.VMEM((2, 2 * HD, HD), F32),
            pltpu.VMEM((2 * HD, HD), F32),
            pltpu.VMEM((4, 2 * HD, HD), F32),
            pltpu.VMEM((2 * HD, HD), F32),
            pltpu.VMEM((4, 2 * HD, HD), F32),
            pltpu.VMEM((N, 8, HD), F32),
            pltpu.VMEM((2, 8, HD), F32),
            dma((3 * NK + 8,)),
            dma,
            dma,
            dma,
            dma((4,)),
            dma,
            dma((4,)),
            dma((N,)),
            dma((2,)),
            pltpu.SemaphoreType.REGULAR,
            pltpu.SemaphoreType.REGULAR,
        ],
        compiler_params=pltpu.CompilerParams(collective_id=0, has_side_effects=True),
    )(
        x,
        wk,
        wv,
        wq,
        wf.T,
        wu.T,
        speeds,
        ceilings,
        jnp.swapaxes(mult, 1, 2),
        jnp.swapaxes(spike, 1, 2),
        up,
        gain.reshape(1, -1),
    )
    return pl.pallas_call(
        place_outputs,
        out_shape=(
            jax.ShapeDtypeStruct((seqs, 1, HD // N, HD), BF16),
            jax.ShapeDtypeStruct((seqs, HD), BF16),
        ),
        in_specs=[vmem],
        out_specs=(vmem, vmem),
    )(near(out))


def solution(mesh):
    placed = (
        P("gr", "sp", None),
        P(None, "tp"),
        P(None, "tp"),
        P(None, "tp"),
        P(),
        P(),
        P("tp"),
        P("tp"),
        P("gr", "sp", "tp"),
        P("gr", "sp", "tp"),
        P("gr", None),
        P(),
    )
    return jax.shard_map(
        on_device,
        mesh=mesh,
        in_specs=placed,
        out_specs=(P("gr", "tp", "sp", None), P("gr", "tp")),
        check_vma=False,
    )
```

```python
import jax
import jax.numpy as jnp
from jax import lax
from jax.experimental import pallas as pl
from jax.experimental.pallas import tpu as pltpu
from jax.sharding import PartitionSpec as P

EPS = 1e-06
F32 = jnp.float32
BF16 = jnp.bfloat16
MESH = pl.DeviceIdType.MESH
NY = 8
NZ = 4
N = NY * NZ
ZR = 3
NK = 4
EARLY = 0
RX0, RX1 = 6, 2
FIRST = (0, 1, 7, 2, 6, 3, 5, 4)
OUT = pltpu.VMEM
CH = 128
HD = 128
NN = (((1,), (0,)), ((), ()))
NT = (((1,), (1,)), ((), ()))


def dot1(a, b, dims=NN):
    return lax.dot_general(a.astype(BF16), b.astype(BF16), dims, preferred_element_type=F32)


def halves(a):
    high = a.astype(BF16)
    return high, (a - high.astype(F32)).astype(BF16)


def dot3(a, b, dims=NN):
    ah, al = halves(a)
    bh, bl = halves(b)
    left = jnp.concatenate([ah, ah, al], axis=1)
    right = jnp.concatenate([bh, bl, bh], axis=dims[0][1][0])
    return lax.dot_general(left, right, dims, preferred_element_type=F32)


def silu(z):
    return z / (1.0 + jnp.exp(-z))


def softplus(z):
    return jnp.maximum(z, 0.0) + jnp.log1p(jnp.exp(-jnp.abs(z)))


def sigmoid(z):
    return 1.0 / (1.0 + jnp.exp(-z))


def unit_rows(z):
    return z * lax.rsqrt(jnp.sum(z * z, axis=-1, keepdims=True) + EPS)


def iota(shape, dim):
    return lax.broadcasted_iota(jnp.int32, shape, dim)


def chunk_maps(keys, values, sums, betas):
    some = range(len(keys))
    rows, cols = iota((CH, CH), 0), iota((CH, CH), 1)
    c_rows = [jnp.transpose(jnp.broadcast_to(c, (CH, CH))) for c in sums]
    ends = [c[:, CH - 1 :] for c in sums]
    match = [dot1(k, k, NT) for k in keys]
    k_t = [jnp.transpose(k) for k in keys]
    v_t = [jnp.transpose(v) for v in values]
    power = [
        jnp.where(cols > rows, match[i] * betas[i] * jnp.exp(sums[i] - c_rows[i]), 0.0)
        for i in some
    ]
    rhs = [
        jnp.concatenate([k_t[i] * (-betas[i] * jnp.exp(sums[i])), v_t[i] * betas[i]], axis=0)
        for i in some
    ]
    for level in range(6):
        both = [dot1(jnp.concatenate([power[i], rhs[i]], axis=0), power[i]) for i in some]
        power = [both[i][:CH] for i in some]
        applied = [both[i][CH:] for i in some]
        rhs = [rhs[i] - applied[i] if level == 0 else rhs[i] + applied[i] for i in some]
    rhs = [rhs[i] + dot1(rhs[i], power[i]) for i in some]
    faded = [keys[i] * jnp.exp(ends[i] - c_rows[i]) for i in some]
    decayed = [jnp.where(rows == cols, jnp.exp(ends[i]), 0.0) for i in some]
    turned = [dot3(rhs[i][:HD], faded[i]) + decayed[i] for i in some]
    whole = dot3(turned[0], turned[1])

    def added():
        parts = [dot3(rhs[i][HD:], faded[i]) for i in some]
        return dot3(parts[0], turned[1]) + parts[1]

    return whole, added


def kernel(
    x_hbm,
    wk_hbm,
    wv_hbm,
    wq_hbm,
    wf_hbm,
    wu_hbm,
    speed_ref,
    ceil_ref,
    mult_hbm,
    spike_hbm,
    up_hbm,
    gain_hbm,
    out_ref,
    xs,
    wkv,
    wqs,
    wfs,
    wus,
    mults,
    spikes,
    ups,
    gains,
    dsc,
    uq,
    uk,
    other_map,
    own_map,
    pair_map,
    row_map,
    row_sum,
    col_map,
    msg,
    fin,
    lsem,
    s1,
    r1,
    s2,
    r2,
    s3,
    r3,
    s4,
    r4,
    row_ready,
    col_ready,
):
    sp = lax.axis_index("sp")
    tp = lax.axis_index("tp")
    y, z = lax.rem(sp, NY), lax.div(sp, NY)
    core = lax.rem(tp, 2)
    par, pair = lax.rem(y, 2), lax.div(y, 2)

    def offset(there):
        return lax.div(lax.rem(there - core + 4, 4) + 1, 2)

    s = lax.rem(par + offset(pair), 2)
    other = 1 - s

    def rx_y(seq):
        return lax.rem(RX0 + (RX1 - RX0) * seq + 2 * core, NY)

    is_rx = y == rx_y(s)
    heads = wf_hbm.shape[0]
    head = lax.rem(tp, heads)

    depth = wk_hbm.shape[0] // NK
    pieces = [pl.ds(i * depth, depth) for i in range(NK)]
    pairs = [(wf_hbm, wfs), (wu_hbm, wus)]
    for piece in pieces:
        pairs += [
            (wk_hbm.at[piece], wkv.at[piece, 0:HD]),
            (wv_hbm.at[piece], wkv.at[piece, HD : 2 * HD]),
            (x_hbm.at[other, :, piece], xs.at[other, :, piece]),
        ]
    pairs += [
        (mult_hbm, mults),
        (spike_hbm, spikes),
        (x_hbm.at[s], xs.at[s]),
        (wq_hbm, wqs),
        (up_hbm, ups),
        (gain_hbm, gains),
    ]
    loads = [pltpu.make_async_copy(a, b, lsem.at[i]) for i, (a, b) in enumerate(pairs)]
    first = 3 * NK + 4
    for load in loads[:first]:
        load.start()

    barrier = pltpu.get_barrier_semaphore()

    def greet(device):
        pl.semaphore_signal(barrier, inc=1, device_id={"sp": device}, device_id_type=MESH)

    partner = sp + 1 - 2 * par
    greet(partner)

    def senders(signal):
        for i in range(1, 4):
            there = lax.rem(pair + i, 4)
            signal(z * NY + 2 * there + lax.rem(s + offset(there), 2))

    @pl.when(is_rx)
    def _():
        @pl.when(z != ZR)
        def _():
            greet(ZR * NY + y)

    @pl.when(jnp.logical_not(is_rx))
    def _():
        greet(z * NY + rx_y(s))

    speed, ceiling = speed_ref[0], ceil_ref[0]
    loads[0].wait()
    loads[1].wait()
    wfu = jnp.concatenate([wfs[...].astype(F32), wus[...].astype(F32)], axis=0).astype(BF16)

    def project(seq, piece):
        x = xs[seq, :, piece]
        raw = lax.dot_general(x, wkv[piece], NN, preferred_element_type=F32)
        pre = lax.dot_general(wfu[:, piece], x, NT, preferred_element_type=F32)
        return raw, pre

    def seq_map(seq, raw, pre):
        dsc[...] = pre
        raw = raw.astype(BF16).astype(F32)
        act = silu(raw)
        k, v = unit_rows(act[:, :HD]), act[:, HD:]
        decay = dsc[pl.ds(head, 1), :]
        strength = dsc[pl.ds(heads + head, 1), :]
        g = -speed * softplus(decay) * mults[seq] + spikes[seq]
        beta = ceiling * sigmoid(strength)
        g_high = g.astype(BF16).astype(F32)
        g_rest = g - g_high
        g_mid = g_rest.astype(BF16).astype(F32)
        g_low = g_rest - g_mid
        row = iota((8, CH), 0)
        parts = jnp.zeros((8, CH), F32)
        place = 0
        for i in range(2):
            for part in (g_high, g_mid, g_low):
                parts = jnp.where(row == place, part[:, i * CH : (i + 1) * CH], parts)
                place += 1
        upper = jnp.where(iota((CH, CH), 0) <= iota((CH, CH), 1), 1.0, 0.0)
        sums = dot1(parts, upper)
        slices = [slice(i * CH, (i + 1) * CH) for i in range(2)]
        return chunk_maps(
            [k[sl] for sl in slices],
            [v[sl] for sl in slices],
            [sums[3 * i : 3 * i + 1] + sums[3 * i + 1 : 3 * i + 2] + sums[3 * i + 2 : 3 * i + 3] for i in range(2)],
            [beta[:, sl] for sl in slices],
        )

    with jax.named_scope("p_seqA"):
        raw, pre = None, None
        for i in range(NK):
            for load in loads[2 + 3 * i : 5 + 3 * i]:
                load.wait()
            if i == NK - 2:
                loads[first].start()
            raw_part, pre_part = project(other, slice(i * depth, (i + 1) * depth))
            raw = raw_part if raw is None else raw + raw_part
            pre = pre_part if pre is None else pre + pre_part
        for load in loads[first + 1 :]:
            load.start()
        for load in loads[first - 2 : first]:
            load.wait()
        whole, added = seq_map(other, raw, pre)
        other_map[0:HD] = whole

    with jax.named_scope("p_barrier"):
        expected = jnp.where(is_rx, jnp.where(z == ZR, 4 + NZ - 1, 4), 1)
        pl.semaphore_wait(barrier, expected)

    @pl.when(is_rx)
    def _():
        def ready(device):
            pl.semaphore_signal(row_ready, inc=1, device_id={"sp": device}, device_id_type=MESH)

        senders(ready)

        @pl.when(z == ZR)
        def _():
            for i in range(NZ):
                if i != ZR:
                    pl.semaphore_signal(
                        col_ready, inc=1, device_id={"sp": i * NY + y}, device_id_type=MESH
                    )

    def swap(part, slot):
        rows = pl.ds(part * HD, HD)
        return pltpu.make_async_remote_copy(
            src_ref=other_map.at[rows],
            dst_ref=own_map.at[slot, rows],
            send_sem=s1.at[part],
            recv_sem=r1.at[part],
            device_id={"sp": partner},
            device_id_type=MESH,
        )

    early = core == EARLY
    pl.when(early)(swap(0, par).start)
    with jax.named_scope("p_seqA2"):
        other_map[HD : 2 * HD] = added()
    pl.when(early)(swap(1, par).start)
    with jax.named_scope("p_seqB"):
        loads[first].wait()
        raw, pre = project(s, slice(0, NK * depth))

    with jax.named_scope("p_seqB2"):
        whole, added = seq_map(s, raw, pre)
        own_map[par, 0:HD] = whole
        own_map[par, HD : 2 * HD] = added()

    @pl.when(jnp.logical_not(early))
    def _():
        swap(0, par).start()
        swap(1, par).start()

    with jax.named_scope("p_r1wait"):
        swap(0, 1 - par).wait_recv()
    with jax.named_scope("p_pair"):
        pair_map[0:HD] = dot3(own_map[0, 0:HD], own_map[1, 0:HD])

    def row_copy(part, slot):
        rows = pl.ds(part * HD, HD)
        return pltpu.make_async_remote_copy(
            src_ref=pair_map.at[rows],
            dst_ref=row_map.at[slot, rows],
            send_sem=s2.at[part],
            recv_sem=r2.at[slot, part],
            device_id={"sp": z * NY + rx_y(s)},
            device_id_type=MESH,
        )

    @pl.when(jnp.logical_not(is_rx))
    def _():
        pl.semaphore_wait(row_ready, 1)
        row_copy(0, pair).start()

    with jax.named_scope("p_r1wait2"):
        swap(1, 1 - par).wait_recv()
    with jax.named_scope("p_pair2"):
        pair_map[HD : 2 * HD] = (
            dot3(own_map[0, HD : 2 * HD], own_map[1, 0:HD]) + own_map[1, HD : 2 * HD]
        )

    @pl.when(jnp.logical_not(is_rx))
    def _():
        row_copy(1, pair).start()

    with jax.named_scope("p_up"):
        for load in loads[first + 1 :]:
            load.wait()
        w_all = wkv[...]
        u = ups[...]
        u_raw = lax.dot_general(u, w_all, NN, preferred_element_type=F32).astype(BF16).astype(F32)
        q_raw = lax.dot_general(u, wqs[...], NN, preferred_element_type=F32).astype(BF16).astype(F32)
        u_pre = lax.dot_general(u, wfu, NT, preferred_element_type=F32)
        lane = iota(u_pre.shape, 1)
        u_decay = jnp.sum(jnp.where(lane == head, u_pre, 0.0), axis=1, keepdims=True)
        u_strength = jnp.sum(jnp.where(lane == heads + head, u_pre, 0.0), axis=1, keepdims=True)
        u_act = silu(u_raw)
        new_k, new_v = unit_rows(u_act[:, :HD]), u_act[:, HD:]
        query = unit_rows(silu(q_raw)) * HD ** (-0.5)
        uq[...] = query
        uk[...] = new_k
    @pl.when(is_rx)
    def _():
        row_map[pair] = pair_map[...]
        with jax.named_scope("p_r2wait"):
            for i in range(1, 4):
                row_copy(0, lax.rem(pair + i, 4)).wait_recv()
        with jax.named_scope("p_rowsum"):
            back = dot3(row_map[2, 0:HD], row_map[3, 0:HD])
            whole = dot3(dot3(row_map[0, 0:HD], row_map[1, 0:HD]), back)
            row_sum[0:HD] = whole

        def col_copy(part, slot):
            rows = pl.ds(part * HD, HD)
            return pltpu.make_async_remote_copy(
                src_ref=row_sum.at[rows],
                dst_ref=col_map.at[slot, rows],
                send_sem=s3.at[part],
                recv_sem=r3.at[slot, part],
                device_id={"sp": ZR * NY + y},
                device_id_type=MESH,
            )

        @pl.when(z != ZR)
        def _():
            pl.semaphore_wait(col_ready, 1)

        @pl.when((z != 0) & (z != ZR))
        def _():
            col_copy(0, z).start()

        with jax.named_scope("p_r2wait2"):
            for i in range(1, 4):
                row_copy(1, lax.rem(pair + i, 4)).wait_recv()
        with jax.named_scope("p_rowsum2"):
            n01 = dot3(row_map[0, HD:], row_map[1, 0:HD]) + row_map[1, HD:]
            n23 = dot3(row_map[2, HD:], row_map[3, 0:HD]) + row_map[3, HD:]
            row_sum[HD:] = dot3(n01, back) + n23

        @pl.when(z != ZR)
        def _():
            col_copy(1, z).start()

        @pl.when((z != 0) & (z != ZR))
        def _():
            col_copy(0, z).wait_send()

        @pl.when(z != ZR)
        def _():
            col_copy(1, z).wait_send()

        @pl.when(z == ZR)
        def _():
            q_row, k_row = uq[pl.ds(s, 1), :], uk[pl.ds(s, 1), :]
            at, lanes = iota((8 * N, HD), 0), iota((8 * N, HD), 1)
            inner = at % 8
            picked = jnp.where((inner < 4) & (lanes == 4 * (at // 8) + inner), 1.0, 0.0)
            picked = jnp.where(inner == 4, q_row, picked)
            picked = jnp.where(inner == 5, k_row, picked)
            last_a = dot3(picked, row_sum[0:HD], NT)
            last_b = dot3(picked, row_sum[HD:], NT)
            with jax.named_scope("p_r3wait01"):
                col_copy(1, 0).wait_recv()
                col_copy(0, 1).wait_recv()
                col_copy(1, 1).wait_recv()
            with jax.named_scope("p_state1"):
                state = dot3(col_map[0, HD:], col_map[1, 0:HD]) + col_map[1, HD:]
            with jax.named_scope("p_r3wait3"):
                col_copy(0, 2).wait_recv()
                state = dot3(state, col_map[2, 0:HD])
                col_copy(1, 2).wait_recv()
            with jax.named_scope("p_state"):
                state = state + col_map[2, HD:]
                msg[...] = (dot3(last_a, state, NT) + last_b).reshape(N, 8, HD)

            def send(to):
                return pltpu.make_async_remote_copy(
                    src_ref=msg.at[to],
                    dst_ref=fin.at[s],
                    send_sem=s4.at[to],
                    recv_sem=r4.at[s],
                    device_id={"sp": to},
                    device_id_type=MESH,
                )

            with jax.named_scope("p_r4send"):
                targets = [i * NY + j for i in range(NZ) for j in FIRST]
                for to in targets:
                    if to // NY == ZR:
                        pl.when(to != sp)(send(to).start)
                    else:
                        send(to).start()
                fin[s] = msg[sp]
            for to in targets:
                if to // NY == ZR:
                    pl.when(to != sp)(send(to).wait_send)
                else:
                    send(to).wait_send()

    for part in range(2):
        swap(part, par).wait_send()

    @pl.when(jnp.logical_not(is_rx))
    def _():
        for part in range(2):
            row_copy(part, pair).wait_send()

    with jax.named_scope("p_r4wait"):
        for seq in range(2):

            @pl.when(ZR * NY + rx_y(seq) != sp)
            def _():
                pltpu.make_async_remote_copy(
                    src_ref=msg.at[0],
                    dst_ref=fin.at[seq],
                    send_sem=s4.at[0],
                    recv_sem=r4.at[seq],
                    device_id={"sp": sp},
                    device_id_type=MESH,
                ).wait_recv()

    with jax.named_scope("p_finish"):
        tiles = [fin[seq] for seq in range(2)]
        query_state = jnp.concatenate([tile[4:5] for tile in tiles], axis=0)
        key_state = jnp.concatenate([tile[5:6] for tile in tiles], axis=0)
        rate = -speed * softplus(u_decay)
        match = jnp.sum(query * new_k, axis=-1, keepdims=True) * (ceiling * sigmoid(u_strength))
        mixed = jnp.exp(rate) * (query_state - match * key_state) + match * new_v
        scale = lax.rsqrt(jnp.mean(mixed * mixed, axis=-1, keepdims=True) + EPS)
        read = mixed * scale * gains[...]
        row = iota((8, HD), 0)
        for seq in range(2):
            out_ref[seq] = jnp.where(row == 4, read[seq : seq + 1], tiles[seq])


def near(a):
    return pltpu.with_memory_space_constraint(a, pltpu.VMEM)


def place_outputs(tiles_ref, cache_ref, read_ref):
    for seq in range(2):
        cache_ref[seq, 0] = tiles_ref[seq, 0:4].astype(BF16)
    rows = [tiles_ref[seq, 4:5] for seq in range(2)]
    read_ref[...] = jnp.concatenate(rows, axis=0).astype(BF16)


def on_device(x, wk, wv, wq, wf, wu, speeds, ceilings, mult, spike, up, gain):
    seqs, span, width = x.shape
    heads = wf.shape[1]
    any_space = pl.BlockSpec(memory_space=pl.ANY)
    smem = pl.BlockSpec(memory_space=pltpu.SMEM)
    vmem = pl.BlockSpec(memory_space=pltpu.VMEM)
    dma = pltpu.SemaphoreType.DMA
    out = pl.pallas_call(
        kernel,
        out_shape=OUT((seqs, 8, HD), F32),
        in_specs=[any_space] * 6 + [smem] * 2 + [any_space] * 4,
        out_specs=vmem,
        scratch_shapes=[
            pltpu.VMEM((seqs, span, width), BF16),
            pltpu.VMEM((width, 2 * HD), BF16),
            pltpu.VMEM((width, HD), BF16),
            pltpu.VMEM((heads, width), BF16),
            pltpu.VMEM((heads, width), BF16),
            pltpu.VMEM((seqs, 1, span), F32),
            pltpu.VMEM((seqs, 1, span), F32),
            pltpu.VMEM((seqs, width), BF16),
            pltpu.VMEM((1, HD), F32),
            pltpu.VMEM((2 * heads, span), F32),
            pltpu.VMEM((seqs, HD), F32),
            pltpu.VMEM((seqs, HD), F32),
            pltpu.VMEM((2 * HD, HD), F32),
            pltpu.VMEM((2, 2 * HD, HD), F32),
            pltpu.VMEM((2 * HD, HD), F32),
            pltpu.VMEM((4, 2 * HD, HD), F32),
            pltpu.VMEM((2 * HD, HD), F32),
            pltpu.VMEM((4, 2 * HD, HD), F32),
            pltpu.VMEM((N, 8, HD), F32),
            pltpu.VMEM((2, 8, HD), F32),
            dma((3 * NK + 8,)),
            dma((2,)),
            dma((2,)),
            dma((2,)),
            dma((4, 2)),
            dma((2,)),
            dma((4, 2)),
            dma((N,)),
            dma((2,)),
            pltpu.SemaphoreType.REGULAR,
            pltpu.SemaphoreType.REGULAR,
        ],
        compiler_params=pltpu.CompilerParams(collective_id=0, has_side_effects=True),
    )(
        x,
        wk,
        wv,
        wq,
        wf.T,
        wu.T,
        speeds,
        ceilings,
        jnp.swapaxes(mult, 1, 2),
        jnp.swapaxes(spike, 1, 2),
        up,
        gain.reshape(1, -1),
    )
    return pl.pallas_call(
        place_outputs,
        out_shape=(
            jax.ShapeDtypeStruct((seqs, 1, HD // N, HD), BF16),
            jax.ShapeDtypeStruct((seqs, HD), BF16),
        ),
        in_specs=[vmem],
        out_specs=(vmem, vmem),
    )(near(out))


def solution(mesh):
    placed = (
        P("gr", "sp", None),
        P(None, "tp"),
        P(None, "tp"),
        P(None, "tp"),
        P(),
        P(),
        P("tp"),
        P("tp"),
        P("gr", "sp", "tp"),
        P("gr", "sp", "tp"),
        P("gr", None),
        P(),
    )
    return jax.shard_map(
        on_device,
        mesh=mesh,
        in_specs=placed,
        out_specs=(P("gr", "tp", "sp", None), P("gr", "tp")),
        check_vma=False,
    )
```

```python
import jax
import jax.numpy as jnp
from jax import lax
from jax.experimental import pallas as pl
from jax.experimental.pallas import tpu as pltpu
from jax.sharding import PartitionSpec as P

EPS = 1e-06
F32 = jnp.float32
BF16 = jnp.bfloat16
MESH = pl.DeviceIdType.MESH
NY = 8
NZ = 4
N = NY * NZ
ZR = 2
NK = 4
EARLY = 0
RX0, RX1 = 6, 2
FIRST = (0, 1, 7, 2, 6, 3, 5, 4)
TARGETS = tuple(i * NY + j for i in (0, 1, 3, 2) for j in FIRST)
OUT = pltpu.VMEM
CH = 128
HD = 128
NN = (((1,), (0,)), ((), ()))
NT = (((1,), (1,)), ((), ()))


def dot1(a, b, dims=NN):
    return lax.dot_general(a.astype(BF16), b.astype(BF16), dims, preferred_element_type=F32)


def halves(a):
    high = a.astype(BF16)
    return high, (a - high.astype(F32)).astype(BF16)


def dot3(a, b, dims=NN):
    ah, al = halves(a)
    bh, bl = halves(b)
    left = jnp.concatenate([ah, ah, al], axis=1)
    right = jnp.concatenate([bh, bl, bh], axis=dims[0][1][0])
    return lax.dot_general(left, right, dims, preferred_element_type=F32)


def silu(z):
    return z / (1.0 + jnp.exp(-z))


def softplus(z):
    return jnp.maximum(z, 0.0) + jnp.log1p(jnp.exp(-jnp.abs(z)))


def sigmoid(z):
    return 1.0 / (1.0 + jnp.exp(-z))


def unit_rows(z):
    return z * lax.rsqrt(jnp.sum(z * z, axis=-1, keepdims=True) + EPS)


def iota(shape, dim):
    return lax.broadcasted_iota(jnp.int32, shape, dim)


def chunk_maps(keys, values, sums, betas):
    some = range(len(keys))
    rows, cols = iota((CH, CH), 0), iota((CH, CH), 1)
    c_rows = [jnp.transpose(jnp.broadcast_to(c, (CH, CH))) for c in sums]
    ends = [c[:, CH - 1 :] for c in sums]
    match = [dot1(k, k, NT) for k in keys]
    k_t = [jnp.transpose(k) for k in keys]
    v_t = [jnp.transpose(v) for v in values]
    power = [
        jnp.where(cols > rows, match[i] * betas[i] * jnp.exp(sums[i] - c_rows[i]), 0.0)
        for i in some
    ]
    rhs = [
        jnp.concatenate([k_t[i] * (-betas[i] * jnp.exp(sums[i])), v_t[i] * betas[i]], axis=0)
        for i in some
    ]
    for level in range(6):
        both = [dot1(jnp.concatenate([power[i], rhs[i]], axis=0), power[i]) for i in some]
        power = [both[i][:CH] for i in some]
        applied = [both[i][CH:] for i in some]
        rhs = [rhs[i] - applied[i] if level == 0 else rhs[i] + applied[i] for i in some]
    rhs = [rhs[i] + dot1(rhs[i], power[i]) for i in some]
    faded = [keys[i] * jnp.exp(ends[i] - c_rows[i]) for i in some]
    decayed = [jnp.where(rows == cols, jnp.exp(ends[i]), 0.0) for i in some]
    turned = [dot3(rhs[i][:HD], faded[i]) + decayed[i] for i in some]
    whole = dot3(turned[0], turned[1])

    def added():
        parts = [dot3(rhs[i][HD:], faded[i]) for i in some]
        return dot3(parts[0], turned[1]) + parts[1]

    return whole, added


def kernel(
    x_hbm,
    wk_hbm,
    wv_hbm,
    wq_hbm,
    wf_hbm,
    wu_hbm,
    speed_ref,
    ceil_ref,
    mult_hbm,
    spike_hbm,
    up_hbm,
    gain_hbm,
    fin,
    aux_out,
    xs,
    wkv,
    wqs,
    wfs,
    wus,
    mults,
    spikes,
    ups,
    gains,
    dsc,
    uq,
    uk,
    other_map,
    own_map,
    pair_map,
    row_map,
    row_sum,
    col_map,
    msg,
    aux,
    lsem,
    s1,
    r1,
    s2,
    r2,
    s3,
    r3,
    s4,
    r4,
    row_ready,
    col_ready,
):
    sp = lax.axis_index("sp")
    tp = lax.axis_index("tp")
    y, z = lax.rem(sp, NY), lax.div(sp, NY)
    core = lax.rem(tp, 2)
    par, pair = lax.rem(y, 2), lax.div(y, 2)

    def offset(there):
        return lax.div(lax.rem(there - core + 4, 4) + 1, 2)

    s = lax.rem(par + offset(pair), 2)
    other = 1 - s

    def rx_y(seq):
        return lax.rem(RX0 + (RX1 - RX0) * seq + 2 * core, NY)

    is_rx = y == rx_y(s)
    heads = wf_hbm.shape[0]
    head = lax.rem(tp, heads)

    depth = wk_hbm.shape[0] // NK
    pieces = [pl.ds(i * depth, depth) for i in range(NK)]
    pairs = [(wf_hbm, wfs, NK), (wu_hbm, wus, NK + 1)]
    for i, piece in enumerate(pieces):
        pairs += [
            (wk_hbm.at[piece], wkv.at[piece, 0:HD], i),
            (wv_hbm.at[piece], wkv.at[piece, HD : 2 * HD], i),
            (x_hbm.at[other, :, piece], xs.at[other, :, piece], i),
        ]
    pairs += [
        (mult_hbm, mults, NK + 2),
        (spike_hbm, spikes, NK + 3),
        (x_hbm.at[s], xs.at[s], 0),
        (wq_hbm, wqs, 1),
        (up_hbm, ups, 2),
        (gain_hbm, gains, 3),
    ]
    loads = [pltpu.make_async_copy(a, b, lsem.at[i]) for a, b, i in pairs]
    first = 3 * NK + 4
    for load in loads[:first]:
        load.start()

    def sent(ref, sem):
        pltpu.make_async_remote_copy(
            src_ref=ref,
            dst_ref=ref,
            send_sem=sem,
            recv_sem=r1.at[0],
            device_id={"sp": sp},
            device_id_type=MESH,
        ).wait_send()

    barrier = pltpu.get_barrier_semaphore()

    def greet(device):
        pl.semaphore_signal(barrier, inc=1, device_id={"sp": device}, device_id_type=MESH)

    partner = sp + 1 - 2 * par
    greet(partner)

    def senders(signal):
        for i in range(1, 4):
            there = lax.rem(pair + i, 4)
            signal(z * NY + 2 * there + lax.rem(s + offset(there), 2))

    @pl.when(is_rx)
    def _():
        @pl.when(z != ZR)
        def _():
            greet(ZR * NY + y)

    @pl.when(jnp.logical_not(is_rx))
    def _():
        greet(z * NY + rx_y(s))

    speed, ceiling = speed_ref[0], ceil_ref[0]
    loads[0].wait()
    loads[1].wait()
    wfu = jnp.concatenate([wfs[...].astype(F32), wus[...].astype(F32)], axis=0).astype(BF16)

    def project(seq, piece):
        x = xs[seq, :, piece]
        raw = lax.dot_general(x, wkv[piece], NN, preferred_element_type=F32)
        pre = lax.dot_general(wfu[:, piece], x, NT, preferred_element_type=F32)
        return raw, pre

    def seq_map(seq, raw, pre):
        dsc[...] = pre
        raw = raw.astype(BF16).astype(F32)
        act = silu(raw)
        k, v = unit_rows(act[:, :HD]), act[:, HD:]
        decay = dsc[pl.ds(head, 1), :]
        strength = dsc[pl.ds(heads + head, 1), :]
        g = -speed * softplus(decay) * mults[seq] + spikes[seq]
        beta = ceiling * sigmoid(strength)
        g_high = g.astype(BF16).astype(F32)
        g_rest = g - g_high
        g_mid = g_rest.astype(BF16).astype(F32)
        g_low = g_rest - g_mid
        row = iota((8, CH), 0)
        parts = jnp.zeros((8, CH), F32)
        place = 0
        for i in range(2):
            for part in (g_high, g_mid, g_low):
                parts = jnp.where(row == place, part[:, i * CH : (i + 1) * CH], parts)
                place += 1
        upper = jnp.where(iota((CH, CH), 0) <= iota((CH, CH), 1), 1.0, 0.0)
        sums = dot1(parts, upper)
        slices = [slice(i * CH, (i + 1) * CH) for i in range(2)]
        return chunk_maps(
            [k[sl] for sl in slices],
            [v[sl] for sl in slices],
            [sums[3 * i : 3 * i + 1] + sums[3 * i + 1 : 3 * i + 2] + sums[3 * i + 2 : 3 * i + 3] for i in range(2)],
            [beta[:, sl] for sl in slices],
        )

    with jax.named_scope("p_seqA"):
        raw, pre = None, None
        for i in range(NK):
            piece = xs.at[other, :, pl.ds(0, 2 * depth)]
            pltpu.make_async_copy(piece, piece, lsem.at[i]).wait()
            if i == NK - 2:
                loads[first].start()
            raw_part, pre_part = project(other, slice(i * depth, (i + 1) * depth))
            raw = raw_part if raw is None else raw + raw_part
            pre = pre_part if pre is None else pre + pre_part
        for load in loads[first + 1 :]:
            load.start()
        for load in loads[first - 2 : first]:
            load.wait()
        whole, added = seq_map(other, raw, pre)
        other_map[0:HD] = whole

    with jax.named_scope("p_barrier"):
        expected = jnp.where(is_rx, jnp.where(z == ZR, 4 + NZ - 1, 4), 1)
        pl.semaphore_wait(barrier, expected)

    @pl.when(is_rx)
    def _():
        def ready(device):
            pl.semaphore_signal(row_ready, inc=1, device_id={"sp": device}, device_id_type=MESH)

        senders(ready)

        @pl.when(z == ZR)
        def _():
            for i in range(1, NZ):
                there = lax.rem(z + i, NZ) * NY + y
                pl.semaphore_signal(
                    col_ready, inc=1, device_id={"sp": there}, device_id_type=MESH
                )

    def swap(part, slot):
        rows = pl.ds(part * HD, HD)
        return pltpu.make_async_remote_copy(
            src_ref=other_map.at[rows],
            dst_ref=own_map.at[slot, rows],
            send_sem=s1,
            recv_sem=r1.at[part],
            device_id={"sp": partner},
            device_id_type=MESH,
        )

    early = core == EARLY
    pl.when(early)(swap(0, par).start)
    with jax.named_scope("p_seqA2"):
        other_map[HD : 2 * HD] = added()
    pl.when(early)(swap(1, par).start)
    with jax.named_scope("p_seqB"):
        loads[first].wait()
        raw, pre = project(s, slice(0, NK * depth))

    with jax.named_scope("p_seqB2"):
        whole, added = seq_map(s, raw, pre)
        own_map[par, 0:HD] = whole
        own_map[par, HD : 2 * HD] = added()

    @pl.when(jnp.logical_not(early))
    def _():
        swap(0, par).start()
        swap(1, par).start()

    with jax.named_scope("p_r1wait"):
        swap(0, 1 - par).wait_recv()
    with jax.named_scope("p_pair"):
        pair_map[0:HD] = dot3(own_map[0, 0:HD], own_map[1, 0:HD])

    def row_copy(part, slot):
        rows = pl.ds(part * HD, HD)
        return pltpu.make_async_remote_copy(
            src_ref=pair_map.at[rows],
            dst_ref=row_map.at[slot, rows],
            send_sem=s2,
            recv_sem=r2.at[slot, part],
            device_id={"sp": z * NY + rx_y(s)},
            device_id_type=MESH,
        )

    @pl.when(jnp.logical_not(is_rx))
    def _():
        pl.semaphore_wait(row_ready, 1)
        row_copy(0, pair).start()

    with jax.named_scope("p_r1wait2"):
        swap(1, 1 - par).wait_recv()
    with jax.named_scope("p_pair2"):
        pair_map[HD : 2 * HD] = (
            dot3(own_map[0, HD : 2 * HD], own_map[1, 0:HD]) + own_map[1, HD : 2 * HD]
        )

    @pl.when(jnp.logical_not(is_rx))
    def _():
        row_copy(1, pair).start()

    with jax.named_scope("p_up"):
        for load in loads[first + 1 :]:
            load.wait()
        w_all = wkv[...]
        u = ups[...]
        u_raw = lax.dot_general(u, w_all, NN, preferred_element_type=F32).astype(BF16).astype(F32)
        q_raw = lax.dot_general(u, wqs[...], NN, preferred_element_type=F32).astype(BF16).astype(F32)
        u_pre = lax.dot_general(u, wfu, NT, preferred_element_type=F32)
        lane = iota(u_pre.shape, 1)
        u_decay = jnp.sum(jnp.where(lane == head, u_pre, 0.0), axis=1, keepdims=True)
        u_strength = jnp.sum(jnp.where(lane == heads + head, u_pre, 0.0), axis=1, keepdims=True)
        u_act = silu(u_raw)
        new_k, new_v = unit_rows(u_act[:, :HD]), u_act[:, HD:]
        query = unit_rows(silu(q_raw)) * HD ** (-0.5)
        uq[...] = query
        uk[...] = new_k
        rate = -speed * softplus(u_decay)
        match = jnp.sum(query * new_k, axis=-1, keepdims=True) * (ceiling * sigmoid(u_strength))
        fading = jnp.exp(rate)
        rows = (fading, fading * match, match * new_v, gains[...])
        for i, value in enumerate(rows):
            aux[i] = jnp.broadcast_to(value, (2, HD))
        aux_copy = pltpu.make_async_copy(aux, aux_out, lsem.at[NK + 1])
        aux_copy.start()

    @pl.when(is_rx)
    def _():
        row_map[pair] = pair_map[...]
        with jax.named_scope("p_r2wait"):
            for i in range(1, 4):
                row_copy(0, lax.rem(pair + i, 4)).wait_recv()
        with jax.named_scope("p_rowsum"):
            back = dot3(row_map[2, 0:HD], row_map[3, 0:HD])
            whole = dot3(dot3(row_map[0, 0:HD], row_map[1, 0:HD]), back)
            row_sum[0:HD] = whole

        def col_copy(part, slot):
            rows = pl.ds(part * HD, HD)
            return pltpu.make_async_remote_copy(
                src_ref=row_sum.at[rows],
                dst_ref=col_map.at[slot, rows],
                send_sem=s3,
                recv_sem=r3.at[slot, part],
                device_id={"sp": ZR * NY + y},
                device_id_type=MESH,
            )

        def run(part, action):
            @pl.when((z != ZR) & (z >= 1 - part))
            def _():
                action(col_copy(part, z))

        @pl.when(z != ZR)
        def _():
            pl.semaphore_wait(col_ready, 1)

        run(0, lambda copy: copy.start())

        with jax.named_scope("p_r2wait2"):
            for i in range(1, 4):
                row_copy(1, lax.rem(pair + i, 4)).wait_recv()
        with jax.named_scope("p_rowsum2"):
            n01 = dot3(row_map[0, HD:], row_map[1, 0:HD]) + row_map[1, HD:]
            n23 = dot3(row_map[2, HD:], row_map[3, 0:HD]) + row_map[3, HD:]
            row_sum[HD:] = dot3(n01, back) + n23

        run(1, lambda copy: copy.start())

        @pl.when(z == ZR)
        def _():
            q_row, k_row = uq[pl.ds(s, 1), :], uk[pl.ds(s, 1), :]
            at, lanes = iota((8 * N, HD), 0), iota((8 * N, HD), 1)
            inner = at % 8
            picked = jnp.where((inner < 4) & (lanes == 4 * (at // 8) + inner), 1.0, 0.0)
            picked = jnp.where(inner == 4, q_row, picked)
            picked = jnp.where(inner == 5, k_row, picked)

            def arrive(part, slot):
                col_copy(part, slot).wait_recv()
                return col_map[slot, part * HD : (part + 1) * HD]

            with jax.named_scope("p_r3wait01"):
                early_b = arrive(1, 0)
                late_a = arrive(0, 1)
                late_b = arrive(1, 1)
            with jax.named_scope("p_state1"):
                state = dot3(early_b, late_a) + late_b
                state = dot3(state, row_sum[0:HD]) + row_sum[HD:]
            with jax.named_scope("p_r3wait3"):
                last_a = dot3(picked, arrive(0, 3), NT)
                late_b = arrive(1, 3)
            with jax.named_scope("p_state"):
                out = dot3(last_a, state, NT) + dot3(picked, late_b, NT)
                msg[...] = out.reshape(N, 8, HD)

            def send(to):
                return pltpu.make_async_remote_copy(
                    src_ref=msg.at[to],
                    dst_ref=fin.at[s],
                    send_sem=s4,
                    recv_sem=r4.at[s],
                    device_id={"sp": to},
                    device_id_type=MESH,
                )

            def each(action):
                for to in TARGETS:
                    if to // NY == ZR:
                        pl.when(to != sp)(lambda: action(send(to)))
                    else:
                        action(send(to))

            each(lambda copy: copy.start())
            own = pltpu.make_async_copy(msg.at[sp], fin.at[s], lsem.at[NK])
            own.start()
            own.wait()
            sent(msg.at[0 : N - 1], s4)

        @pl.when(z == 0)
        def _():
            sent(row_sum.at[0:HD], s3)

        @pl.when((z != 0) & (z != ZR))
        def _():
            sent(row_sum, s3)

    sent(other_map, s1)

    @pl.when(jnp.logical_not(is_rx))
    def _():
        sent(pair_map, s2)

    with jax.named_scope("p_r4wait"):
        for seq in range(2):

            @pl.when(ZR * NY + rx_y(seq) != sp)
            def _():
                pltpu.make_async_remote_copy(
                    src_ref=msg.at[0],
                    dst_ref=fin.at[seq],
                    send_sem=s4,
                    recv_sem=r4.at[seq],
                    device_id={"sp": sp},
                    device_id_type=MESH,
                ).wait_recv()

    aux_copy.wait()


def near(a):
    return pltpu.with_memory_space_constraint(a, pltpu.VMEM)


def place_outputs(fin_ref, aux_ref, cache_ref, read_ref):
    tiles = [fin_ref[seq] for seq in range(2)]
    for seq in range(2):
        cache_ref[seq, 0] = tiles[seq][0:4].astype(BF16)
    query_state = jnp.concatenate([tile[4:5] for tile in tiles], axis=0)
    key_state = jnp.concatenate([tile[5:6] for tile in tiles], axis=0)
    mixed = aux_ref[0] * query_state - aux_ref[1] * key_state + aux_ref[2]
    scale = lax.rsqrt(jnp.mean(mixed * mixed, axis=-1, keepdims=True) + EPS)
    read_ref[...] = (mixed * scale * aux_ref[3]).astype(BF16)


def on_device(x, wk, wv, wq, wf, wu, speeds, ceilings, mult, spike, up, gain):
    seqs, span, width = x.shape
    heads = wf.shape[1]
    any_space = pl.BlockSpec(memory_space=pl.ANY)
    smem = pl.BlockSpec(memory_space=pltpu.SMEM)
    vmem = pl.BlockSpec(memory_space=pltpu.VMEM)
    dma = pltpu.SemaphoreType.DMA
    out = pl.pallas_call(
        kernel,
        out_shape=(OUT((seqs, 8, HD), F32), OUT((4, seqs, HD), F32)),
        in_specs=[any_space] * 6 + [smem] * 2 + [any_space] * 4,
        out_specs=(any_space, any_space),
        scratch_shapes=[
            pltpu.VMEM((seqs, span, width), BF16),
            pltpu.VMEM((width, 2 * HD), BF16),
            pltpu.VMEM((width, HD), BF16),
            pltpu.VMEM((heads, width), BF16),
            pltpu.VMEM((heads, width), BF16),
            pltpu.VMEM((seqs, 1, span), F32),
            pltpu.VMEM((seqs, 1, span), F32),
            pltpu.VMEM((seqs, width), BF16),
            pltpu.VMEM((1, HD), F32),
            pltpu.VMEM((2 * heads, span), F32),
            pltpu.VMEM((seqs, HD), F32),
            pltpu.VMEM((seqs, HD), F32),
            pltpu.VMEM((2 * HD, HD), F32),
            pltpu.VMEM((2, 2 * HD, HD), F32),
            pltpu.VMEM((2 * HD, HD), F32),
            pltpu.VMEM((4, 2 * HD, HD), F32),
            pltpu.VMEM((2 * HD, HD), F32),
            pltpu.VMEM((4, 2 * HD, HD), F32),
            pltpu.VMEM((N, 8, HD), F32),
            pltpu.VMEM((4, seqs, HD), F32),
            dma((NK + 4,)),
            dma,
            dma((2,)),
            dma,
            dma((4, 2)),
            dma,
            dma((4, 2)),
            dma,
            dma((2,)),
            pltpu.SemaphoreType.REGULAR,
            pltpu.SemaphoreType.REGULAR,
        ],
        compiler_params=pltpu.CompilerParams(collective_id=0, has_side_effects=True),
    )(
        x,
        wk,
        wv,
        wq,
        wf.T,
        wu.T,
        speeds,
        ceilings,
        jnp.swapaxes(mult, 1, 2),
        jnp.swapaxes(spike, 1, 2),
        up,
        gain.reshape(1, -1),
    )
    return pl.pallas_call(
        place_outputs,
        out_shape=(
            jax.ShapeDtypeStruct((seqs, 1, HD // N, HD), BF16),
            jax.ShapeDtypeStruct((seqs, HD), BF16),
        ),
        in_specs=[vmem, vmem],
        out_specs=(vmem, vmem),
    )(near(out[0]), near(out[1]))


def solution(mesh):
    placed = (
        P("gr", "sp", None),
        P(None, "tp"),
        P(None, "tp"),
        P(None, "tp"),
        P(),
        P(),
        P("tp"),
        P("tp"),
        P("gr", "sp", "tp"),
        P("gr", "sp", "tp"),
        P("gr", None),
        P(),
    )
    return jax.shard_map(
        on_device,
        mesh=mesh,
        in_specs=placed,
        out_specs=(P("gr", "tp", "sp", None), P("gr", "tp")),
        check_vma=False,
    )
```

```python
import jax
import jax.numpy as jnp
from jax import lax
from jax.experimental import pallas as pl
from jax.experimental.pallas import tpu as pltpu
from jax.sharding import PartitionSpec as P

EPS = 1e-06
F32 = jnp.float32
BF16 = jnp.bfloat16
MESH = pl.DeviceIdType.MESH
NY = 8
NZ = 4
N = NY * NZ
ZR = 2
NK = 4
EARLY = 0
RX0, RX1 = 6, 2
FIRST = (0, 1, 7, 2, 6, 3, 5, 4)
TARGETS = tuple(i * NY + j for i in (0, 1, 3, 2) for j in FIRST)
OUT = pltpu.VMEM
CH = 128
HD = 128
NN = (((1,), (0,)), ((), ()))
NT = (((1,), (1,)), ((), ()))


def dot1(a, b, dims=NN):
    return lax.dot_general(a.astype(BF16), b.astype(BF16), dims, preferred_element_type=F32)


def halves(a):
    high = a.astype(BF16)
    return high, (a - high.astype(F32)).astype(BF16)


def dot3(a, b, dims=NN):
    ah, al = halves(a)
    bh, bl = halves(b)
    left = jnp.concatenate([ah, ah, al], axis=1)
    right = jnp.concatenate([bh, bl, bh], axis=dims[0][1][0])
    return lax.dot_general(left, right, dims, preferred_element_type=F32)


def silu(z):
    return z / (1.0 + jnp.exp(-z))


def softplus(z):
    return jnp.maximum(z, 0.0) + jnp.log1p(jnp.exp(-jnp.abs(z)))


def sigmoid(z):
    return 1.0 / (1.0 + jnp.exp(-z))


def unit_rows(z):
    return z * lax.rsqrt(jnp.sum(z * z, axis=-1, keepdims=True) + EPS)


def iota(shape, dim):
    return lax.broadcasted_iota(jnp.int32, shape, dim)


def chunk_maps(keys, values, sums, betas):
    some = range(len(keys))
    rows, cols = iota((CH, CH), 0), iota((CH, CH), 1)
    c_rows = [jnp.transpose(jnp.broadcast_to(c, (CH, CH))) for c in sums]
    ends = [c[:, CH - 1 :] for c in sums]
    match = [dot3(k, k, NT) for k in keys]
    k_t = [jnp.transpose(k) for k in keys]
    v_t = [jnp.transpose(v) for v in values]
    power = [
        jnp.where(cols > rows, match[i] * betas[i] * jnp.exp(sums[i] - c_rows[i]), 0.0)
        for i in some
    ]
    rhs = [
        jnp.concatenate([k_t[i] * (-betas[i] * jnp.exp(sums[i])), v_t[i] * betas[i]], axis=0)
        for i in some
    ]
    for level in range(6):
        both = [dot3(jnp.concatenate([power[i], rhs[i]], axis=0), power[i]) for i in some]
        power = [both[i][:CH] for i in some]
        applied = [both[i][CH:] for i in some]
        rhs = [rhs[i] - applied[i] if level == 0 else rhs[i] + applied[i] for i in some]
    rhs = [rhs[i] + dot3(rhs[i], power[i]) for i in some]
    faded = [keys[i] * jnp.exp(ends[i] - c_rows[i]) for i in some]
    decayed = [jnp.where(rows == cols, jnp.exp(ends[i]), 0.0) for i in some]
    turned = [dot3(rhs[i][:HD], faded[i]) + decayed[i] for i in some]
    whole = dot3(turned[0], turned[1])

    def added():
        parts = [dot3(rhs[i][HD:], faded[i]) for i in some]
        return dot3(parts[0], turned[1]) + parts[1]

    return whole, added


def kernel(
    x_hbm,
    wk_hbm,
    wv_hbm,
    wq_hbm,
    wf_hbm,
    wu_hbm,
    speed_ref,
    ceil_ref,
    mult_hbm,
    spike_hbm,
    up_hbm,
    gain_hbm,
    fin,
    aux_out,
    xs,
    wkv,
    wqs,
    wfs,
    wus,
    mults,
    spikes,
    ups,
    gains,
    dsc,
    uq,
    uk,
    other_map,
    own_map,
    pair_map,
    row_map,
    row_sum,
    col_map,
    msg,
    aux,
    lsem,
    s1,
    r1,
    s2,
    r2,
    s3,
    r3,
    s4,
    r4,
    row_ready,
    col_ready,
):
    sp = lax.axis_index("sp")
    tp = lax.axis_index("tp")
    y, z = lax.rem(sp, NY), lax.div(sp, NY)
    core = lax.rem(tp, 2)
    par, pair = lax.rem(y, 2), lax.div(y, 2)

    def offset(there):
        return lax.div(lax.rem(there - core + 4, 4) + 1, 2)

    s = lax.rem(par + offset(pair), 2)
    other = 1 - s

    def rx_y(seq):
        return lax.rem(RX0 + (RX1 - RX0) * seq + 2 * core, NY)

    is_rx = y == rx_y(s)
    heads = wf_hbm.shape[0]
    head = lax.rem(tp, heads)

    depth = wk_hbm.shape[0] // NK
    pieces = [pl.ds(i * depth, depth) for i in range(NK)]
    pairs = [(wf_hbm, wfs, NK), (wu_hbm, wus, NK + 1)]
    for i, piece in enumerate(pieces):
        pairs += [
            (wk_hbm.at[piece], wkv.at[piece, 0:HD], i),
            (wv_hbm.at[piece], wkv.at[piece, HD : 2 * HD], i),
            (x_hbm.at[other, :, piece], xs.at[other, :, piece], i),
        ]
    pairs += [
        (mult_hbm, mults, NK + 2),
        (spike_hbm, spikes, NK + 3),
        (x_hbm.at[s], xs.at[s], 0),
        (wq_hbm, wqs, 1),
        (up_hbm, ups, 2),
        (gain_hbm, gains, 3),
    ]
    loads = [pltpu.make_async_copy(a, b, lsem.at[i]) for a, b, i in pairs]
    first = 3 * NK + 4
    for load in loads[:first]:
        load.start()

    def sent(ref, sem):
        pltpu.make_async_remote_copy(
            src_ref=ref,
            dst_ref=ref,
            send_sem=sem,
            recv_sem=r1.at[0],
            device_id={"sp": sp},
            device_id_type=MESH,
        ).wait_send()

    barrier = pltpu.get_barrier_semaphore()

    def greet(device):
        pl.semaphore_signal(barrier, inc=1, device_id={"sp": device}, device_id_type=MESH)

    partner = sp + 1 - 2 * par
    greet(partner)

    def senders(signal):
        for i in range(1, 4):
            there = lax.rem(pair + i, 4)
            signal(z * NY + 2 * there + lax.rem(s + offset(there), 2))

    @pl.when(is_rx)
    def _():
        @pl.when(z != ZR)
        def _():
            greet(ZR * NY + y)

    @pl.when(jnp.logical_not(is_rx))
    def _():
        greet(z * NY + rx_y(s))

    speed, ceiling = speed_ref[0], ceil_ref[0]
    loads[0].wait()
    loads[1].wait()
    wfu = jnp.concatenate([wfs[...].astype(F32), wus[...].astype(F32)], axis=0).astype(BF16)

    def project(seq, piece):
        x = xs[seq, :, piece]
        raw = lax.dot_general(x, wkv[piece], NN, preferred_element_type=F32)
        pre = lax.dot_general(wfu[:, piece], x, NT, preferred_element_type=F32)
        return raw, pre

    def seq_map(seq, raw, pre):
        dsc[...] = pre
        raw = raw.astype(BF16).astype(F32)
        act = silu(raw)
        k, v = unit_rows(act[:, :HD]), act[:, HD:]
        decay = dsc[pl.ds(head, 1), :]
        strength = dsc[pl.ds(heads + head, 1), :]
        g = -speed * softplus(decay) * mults[seq] + spikes[seq]
        beta = ceiling * sigmoid(strength)
        g_high = g.astype(BF16).astype(F32)
        g_rest = g - g_high
        g_mid = g_rest.astype(BF16).astype(F32)
        g_low = g_rest - g_mid
        row = iota((8, CH), 0)
        parts = jnp.zeros((8, CH), F32)
        place = 0
        for i in range(2):
            for part in (g_high, g_mid, g_low):
                parts = jnp.where(row == place, part[:, i * CH : (i + 1) * CH], parts)
                place += 1
        upper = jnp.where(iota((CH, CH), 0) <= iota((CH, CH), 1), 1.0, 0.0)
        sums = dot1(parts, upper)
        slices = [slice(i * CH, (i + 1) * CH) for i in range(2)]
        return chunk_maps(
            [k[sl] for sl in slices],
            [v[sl] for sl in slices],
            [sums[3 * i : 3 * i + 1] + sums[3 * i + 1 : 3 * i + 2] + sums[3 * i + 2 : 3 * i + 3] for i in range(2)],
            [beta[:, sl] for sl in slices],
        )

    with jax.named_scope("p_seqA"):
        raw, pre = None, None
        for i in range(NK):
            piece = xs.at[other, :, pl.ds(0, 2 * depth)]
            pltpu.make_async_copy(piece, piece, lsem.at[i]).wait()
            if i == NK - 2:
                loads[first].start()
            raw_part, pre_part = project(other, slice(i * depth, (i + 1) * depth))
            raw = raw_part if raw is None else raw + raw_part
            pre = pre_part if pre is None else pre + pre_part
        for load in loads[first + 1 :]:
            load.start()
        for load in loads[first - 2 : first]:
            load.wait()
        whole, added = seq_map(other, raw, pre)
        other_map[0:HD] = whole

    with jax.named_scope("p_barrier"):
        expected = jnp.where(is_rx, jnp.where(z == ZR, 4 + NZ - 1, 4), 1)
        pl.semaphore_wait(barrier, expected)

    @pl.when(is_rx)
    def _():
        def ready(device):
            pl.semaphore_signal(row_ready, inc=1, device_id={"sp": device}, device_id_type=MESH)

        senders(ready)

        @pl.when(z == ZR)
        def _():
            for i in range(1, NZ):
                there = lax.rem(z + i, NZ) * NY + y
                pl.semaphore_signal(
                    col_ready, inc=1, device_id={"sp": there}, device_id_type=MESH
                )

    def swap(part, slot):
        rows = pl.ds(part * HD, HD)
        return pltpu.make_async_remote_copy(
            src_ref=other_map.at[rows],
            dst_ref=own_map.at[slot, rows],
            send_sem=s1,
            recv_sem=r1.at[part],
            device_id={"sp": partner},
            device_id_type=MESH,
        )

    early = core == EARLY
    pl.when(early)(swap(0, par).start)
    with jax.named_scope("p_seqA2"):
        other_map[HD : 2 * HD] = added()
    pl.when(early)(swap(1, par).start)
    with jax.named_scope("p_seqB"):
        loads[first].wait()
        raw, pre = project(s, slice(0, NK * depth))

    with jax.named_scope("p_seqB2"):
        whole, added = seq_map(s, raw, pre)
        own_map[par, 0:HD] = whole
        own_map[par, HD : 2 * HD] = added()

    @pl.when(jnp.logical_not(early))
    def _():
        swap(0, par).start()
        swap(1, par).start()

    with jax.named_scope("p_r1wait"):
        swap(0, 1 - par).wait_recv()
    with jax.named_scope("p_pair"):
        pair_map[0:HD] = dot3(own_map[0, 0:HD], own_map[1, 0:HD])

    def row_copy(part, slot):
        rows = pl.ds(part * HD, HD)
        return pltpu.make_async_remote_copy(
            src_ref=pair_map.at[rows],
            dst_ref=row_map.at[slot, rows],
            send_sem=s2,
            recv_sem=r2.at[slot, part],
            device_id={"sp": z * NY + rx_y(s)},
            device_id_type=MESH,
        )

    @pl.when(jnp.logical_not(is_rx))
    def _():
        pl.semaphore_wait(row_ready, 1)
        row_copy(0, pair).start()

    with jax.named_scope("p_r1wait2"):
        swap(1, 1 - par).wait_recv()
    with jax.named_scope("p_pair2"):
        pair_map[HD : 2 * HD] = (
            dot3(own_map[0, HD : 2 * HD], own_map[1, 0:HD]) + own_map[1, HD : 2 * HD]
        )

    @pl.when(jnp.logical_not(is_rx))
    def _():
        row_copy(1, pair).start()

    with jax.named_scope("p_up"):
        for load in loads[first + 1 :]:
            load.wait()
        w_all = wkv[...]
        u = ups[...]
        u_raw = lax.dot_general(u, w_all, NN, preferred_element_type=F32).astype(BF16).astype(F32)
        q_raw = lax.dot_general(u, wqs[...], NN, preferred_element_type=F32).astype(BF16).astype(F32)
        u_pre = lax.dot_general(u, wfu, NT, preferred_element_type=F32)
        lane = iota(u_pre.shape, 1)
        u_decay = jnp.sum(jnp.where(lane == head, u_pre, 0.0), axis=1, keepdims=True)
        u_strength = jnp.sum(jnp.where(lane == heads + head, u_pre, 0.0), axis=1, keepdims=True)
        u_act = silu(u_raw)
        new_k, new_v = unit_rows(u_act[:, :HD]), u_act[:, HD:]
        query = unit_rows(silu(q_raw)) * HD ** (-0.5)
        uq[...] = query
        uk[...] = new_k
        rate = -speed * softplus(u_decay)
        match = jnp.sum(query * new_k, axis=-1, keepdims=True) * (ceiling * sigmoid(u_strength))
        fading = jnp.exp(rate)
        rows = (fading, fading * match, match * new_v, gains[...])
        for i, value in enumerate(rows):
            aux[i] = jnp.broadcast_to(value, (2, HD))
        aux_copy = pltpu.make_async_copy(aux, aux_out, lsem.at[NK + 1])
        aux_copy.start()

    @pl.when(is_rx)
    def _():
        row_map[pair] = pair_map[...]
        with jax.named_scope("p_r2wait"):
            for i in range(1, 4):
                row_copy(0, lax.rem(pair + i, 4)).wait_recv()
        with jax.named_scope("p_rowsum"):
            back = dot3(row_map[2, 0:HD], row_map[3, 0:HD])
            whole = dot3(dot3(row_map[0, 0:HD], row_map[1, 0:HD]), back)
            row_sum[0:HD] = whole

        def col_copy(part, slot):
            rows = pl.ds(part * HD, HD)
            return pltpu.make_async_remote_copy(
                src_ref=row_sum.at[rows],
                dst_ref=col_map.at[slot, rows],
                send_sem=s3,
                recv_sem=r3.at[slot, part],
                device_id={"sp": ZR * NY + y},
                device_id_type=MESH,
            )

        def run(part, action):
            @pl.when((z != ZR) & (z >= 1 - part))
            def _():
                action(col_copy(part, z))

        @pl.when(z != ZR)
        def _():
            pl.semaphore_wait(col_ready, 1)

        run(0, lambda copy: copy.start())

        with jax.named_scope("p_r2wait2"):
            for i in range(1, 4):
                row_copy(1, lax.rem(pair + i, 4)).wait_recv()
        with jax.named_scope("p_rowsum2"):
            n01 = dot3(row_map[0, HD:], row_map[1, 0:HD]) + row_map[1, HD:]
            n23 = dot3(row_map[2, HD:], row_map[3, 0:HD]) + row_map[3, HD:]
            row_sum[HD:] = dot3(n01, back) + n23

        run(1, lambda copy: copy.start())

        @pl.when(z == ZR)
        def _():
            q_row, k_row = uq[pl.ds(s, 1), :], uk[pl.ds(s, 1), :]
            at, lanes = iota((8 * N, HD), 0), iota((8 * N, HD), 1)
            inner = at % 8
            picked = jnp.where((inner < 4) & (lanes == 4 * (at // 8) + inner), 1.0, 0.0)
            picked = jnp.where(inner == 4, q_row, picked)
            picked = jnp.where(inner == 5, k_row, picked)

            def arrive(part, slot):
                col_copy(part, slot).wait_recv()
                return col_map[slot, part * HD : (part + 1) * HD]

            with jax.named_scope("p_r3wait01"):
                early_b = arrive(1, 0)
                late_a = arrive(0, 1)
                late_b = arrive(1, 1)
            with jax.named_scope("p_state1"):
                state = dot3(early_b, late_a) + late_b
                state = dot3(state, row_sum[0:HD]) + row_sum[HD:]
            with jax.named_scope("p_r3wait3"):
                last_a = dot3(picked, arrive(0, 3), NT)
                late_b = arrive(1, 3)
            with jax.named_scope("p_state"):
                out = dot3(last_a, state, NT) + dot3(picked, late_b, NT)
                msg[...] = out.reshape(N, 8, HD)

            def send(to):
                return pltpu.make_async_remote_copy(
                    src_ref=msg.at[to],
                    dst_ref=fin.at[s],
                    send_sem=s4,
                    recv_sem=r4.at[s],
                    device_id={"sp": to},
                    device_id_type=MESH,
                )

            def each(action):
                for to in TARGETS:
                    if to // NY == ZR:
                        pl.when(to != sp)(lambda: action(send(to)))
                    else:
                        action(send(to))

            each(lambda copy: copy.start())
            own = pltpu.make_async_copy(msg.at[sp], fin.at[s], lsem.at[NK])
            own.start()
            own.wait()
            sent(msg.at[0 : N - 1], s4)

        @pl.when(z == 0)
        def _():
            sent(row_sum.at[0:HD], s3)

        @pl.when((z != 0) & (z != ZR))
        def _():
            sent(row_sum, s3)

    sent(other_map, s1)

    @pl.when(jnp.logical_not(is_rx))
    def _():
        sent(pair_map, s2)

    with jax.named_scope("p_r4wait"):
        for seq in range(2):

            @pl.when(ZR * NY + rx_y(seq) != sp)
            def _():
                pltpu.make_async_remote_copy(
                    src_ref=msg.at[0],
                    dst_ref=fin.at[seq],
                    send_sem=s4,
                    recv_sem=r4.at[seq],
                    device_id={"sp": sp},
                    device_id_type=MESH,
                ).wait_recv()

    aux_copy.wait()


def near(a):
    return pltpu.with_memory_space_constraint(a, pltpu.VMEM)


def place_outputs(fin_ref, aux_ref, cache_ref, read_ref):
    tiles = [fin_ref[seq] for seq in range(2)]
    for seq in range(2):
        cache_ref[seq, 0] = tiles[seq][0:4].astype(BF16)
    query_state = jnp.concatenate([tile[4:5] for tile in tiles], axis=0)
    key_state = jnp.concatenate([tile[5:6] for tile in tiles], axis=0)
    mixed = aux_ref[0] * query_state - aux_ref[1] * key_state + aux_ref[2]
    scale = lax.rsqrt(jnp.mean(mixed * mixed, axis=-1, keepdims=True) + EPS)
    read_ref[...] = (mixed * scale * aux_ref[3]).astype(BF16)


def on_device(x, wk, wv, wq, wf, wu, speeds, ceilings, mult, spike, up, gain):
    seqs, span, width = x.shape
    heads = wf.shape[1]
    any_space = pl.BlockSpec(memory_space=pl.ANY)
    smem = pl.BlockSpec(memory_space=pltpu.SMEM)
    vmem = pl.BlockSpec(memory_space=pltpu.VMEM)
    dma = pltpu.SemaphoreType.DMA
    out = pl.pallas_call(
        kernel,
        out_shape=(OUT((seqs, 8, HD), F32), OUT((4, seqs, HD), F32)),
        in_specs=[any_space] * 6 + [smem] * 2 + [any_space] * 4,
        out_specs=(any_space, any_space),
        scratch_shapes=[
            pltpu.VMEM((seqs, span, width), BF16),
            pltpu.VMEM((width, 2 * HD), BF16),
            pltpu.VMEM((width, HD), BF16),
            pltpu.VMEM((heads, width), BF16),
            pltpu.VMEM((heads, width), BF16),
            pltpu.VMEM((seqs, 1, span), F32),
            pltpu.VMEM((seqs, 1, span), F32),
            pltpu.VMEM((seqs, width), BF16),
            pltpu.VMEM((1, HD), F32),
            pltpu.VMEM((2 * heads, span), F32),
            pltpu.VMEM((seqs, HD), F32),
            pltpu.VMEM((seqs, HD), F32),
            pltpu.VMEM((2 * HD, HD), F32),
            pltpu.VMEM((2, 2 * HD, HD), F32),
            pltpu.VMEM((2 * HD, HD), F32),
            pltpu.VMEM((4, 2 * HD, HD), F32),
            pltpu.VMEM((2 * HD, HD), F32),
            pltpu.VMEM((4, 2 * HD, HD), F32),
            pltpu.VMEM((N, 8, HD), F32),
            pltpu.VMEM((4, seqs, HD), F32),
            dma((NK + 4,)),
            dma,
            dma((2,)),
            dma,
            dma((4, 2)),
            dma,
            dma((4, 2)),
            dma,
            dma((2,)),
            pltpu.SemaphoreType.REGULAR,
            pltpu.SemaphoreType.REGULAR,
        ],
        compiler_params=pltpu.CompilerParams(collective_id=0, has_side_effects=True),
    )(
        x,
        wk,
        wv,
        wq,
        wf.T,
        wu.T,
        speeds,
        ceilings,
        jnp.swapaxes(mult, 1, 2),
        jnp.swapaxes(spike, 1, 2),
        up,
        gain.reshape(1, -1),
    )
    return pl.pallas_call(
        place_outputs,
        out_shape=(
            jax.ShapeDtypeStruct((seqs, 1, HD // N, HD), BF16),
            jax.ShapeDtypeStruct((seqs, HD), BF16),
        ),
        in_specs=[vmem, vmem],
        out_specs=(vmem, vmem),
    )(near(out[0]), near(out[1]))


def solution(mesh):
    placed = (
        P("gr", "sp", None),
        P(None, "tp"),
        P(None, "tp"),
        P(None, "tp"),
        P(),
        P(),
        P("tp"),
        P("tp"),
        P("gr", "sp", "tp"),
        P("gr", "sp", "tp"),
        P("gr", None),
        P(),
    )
    return jax.shard_map(
        on_device,
        mesh=mesh,
        in_specs=placed,
        out_specs=(P("gr", "tp", "sp", None), P("gr", "tp")),
        check_vma=False,
    )
```
